256 devices in a mesh: sp: 64 (over z, x, core), tp: 4 (over y).
Axes of the slice: x: 4, y: 4, z: 8, core: 2. Of those that a mesh axis runs over, the one named last changes fastest.
Arguments:
- layer_input: bfloat16 [8192, 2048], P('sp', 'tp'), may hold values from -6 to 6
- cotangent: bfloat16 [8192, 2048], P('sp', 'tp'), may hold values from -16 to 16
- routes: int32 [8192, 2], P('sp'), may hold values from 0 to 63, all different within a row; in each aligned block of 128 rows (0 to 127, 128 to 255, ...) at most 6 rows name the same one
- route_weight: float32 [8192, 2], P('sp'), may hold values from 0.1 to 0.6
- gate_weight: bfloat16 [64, 2048, 1024], P('sp', None, 'tp'), may hold values from -0.125 to 0.125
- up_weight: bfloat16 [64, 2048, 1024], P('sp', None, 'tp'), may hold values from -0.125 to 0.125
- down_weight: bfloat16 [64, 1024, 2048], P('sp', 'tp'), may hold values from -0.1875 to 0.1875
- heads_value: bfloat16 [8192, 2048], P('sp', 'tp'), may hold values from -6 to 6
- output_gate: bfloat16 [8192, 2048], P('sp', 'tp'), may hold values from -8 to 8
- mixer_saved: bfloat16 [8192, 2048], P('sp', 'tp'), may hold values from -6 to 6
- proj_weight: bfloat16 [2048, 2048], P(None, 'tp'), may hold values from -0.125 to 0.125
- state_write: bfloat16 [8192, 512], P('sp', 'tp'), may hold values from -0.5 to 0.5
- state_read: bfloat16 [8192, 512], P('sp', 'tp'), may hold values from -0.5 to 0.5
- decay_rate: float32 [8192, 32], P('sp', 'tp'), may hold values from 0 to 1.1, as said below
Outputs:
- gate_grad: bfloat16 [64, 2048, 1024], P('sp', None, 'tp')
- up_grad: bfloat16 [64, 2048, 1024], P('sp', None, 'tp')
- down_grad: bfloat16 [64, 1024, 2048], P('sp', 'tp')
- proj_grad: float32 [2048, 2048], P('sp', 'tp')
- value_grad: bfloat16 [8192, 2048], P('sp', 'tp')
- write_gradient: bfloat16 [8192, 512], P('sp', 'tp')
- read_gradient: bfloat16 [8192, 512], P('sp', 'tp')
- outgate_grad: bfloat16 [8192, 2048], P('sp', 'tp')
The draws below stay inside these ranges and needn't reach their ends.
Inputs may be any that keep to these rules, and one draw needn't show every extreme that they name: `routes`: each row names 2 different experts; within the rows of one aligned block of 128 tokens no expert is named by more than 6 rows, a bound that some block reaches. `decay_rate`: positive log-decays.
All inputs are finite; a program needn't handle non-finite values.
Results may differ from the reference program's by a relative error of at most 0.017.
Values may be sent and summed in bfloat16 or wider, within the bound.
A program may use at most 128 MiB of HBM per device.

```python
import math
import jax
import jax.numpy as jnp
import numpy as np
from jax import lax

D = 2048
BLENDER_CHANNEL = 32
HEAD_DIM = 64
GROUPS = 4
STATE = 128
EXP_HIDDEN = 1024
TOPK = 2
TOK_DEV = 128
SERIES_ENTRIES = 8192
EXPERTS = 64
CAP = 6
SSD_W = 2048
N_SP = 64
N_TP = 4


def draw_decay_rate(key, part):
    address_rows = jax.random.split(jax.random.fold_in(key, 11), 5)
    share = 0.5
    fast_heads = jax.random.uniform(address_rows[0], (BLENDER_CHANNEL,), jnp.float32) < share
    random_noise = jax.random.uniform(address_rows[1], (SERIES_ENTRIES, BLENDER_CHANNEL), jnp.float32, 0.5, 1.5)
    block_multiplier = jax.random.uniform(address_rows[2], (SERIES_ENTRIES // TOK_DEV, 1, 1), jnp.float32, 0.5, 1.5)
    block_multiplier = jnp.broadcast_to(block_multiplier, (SERIES_ENTRIES // TOK_DEV, TOK_DEV, 1)).reshape(SERIES_ENTRIES, 1)
    baseline_rate = jnp.where(fast_heads, 0.03, 0.5 / SERIES_ENTRIES)[None, :]
    interval_starts = jax.random.randint(address_rows[3], (2, BLENDER_CHANNEL), 0, SERIES_ENTRIES)
    interval_spans = jax.random.uniform(address_rows[4], (2, BLENDER_CHANNEL), jnp.float32, 0.22, 0.5)
    entry_indices = jnp.arange(SERIES_ENTRIES, dtype=jnp.int32)[:, None]
    pulse_clusters = jnp.where(entry_indices == interval_starts[0][None, :], interval_spans[0][None, :], 0.0)
    pulse_clusters = pulse_clusters + jnp.where(entry_indices == interval_starts[1][None, :], interval_spans[1][None, :], 0.0)
    pulse_clusters = jnp.where(fast_heads[None, :], 0.0, pulse_clusters)
    return (baseline_rate * random_noise * block_multiplier + pulse_clusters).astype(jnp.float32)


def raised(result, rng, source, target, shards_of, factor):
    def block_of(dim):
        return (jnp.arange(result.shape[dim]) // (result.shape[dim] // shards_of)).reshape((-1,) + (1,) * (result.ndim - 1 - dim))

    first = jax.random.permutation(rng, shards_of)[block_of(target)]
    second = (block_of(target) + shards_of // 2) % shards_of
    return jnp.where((block_of(source) == first) | (block_of(source) == second), factor * result, result)


def steps_of(rng, shape, cuts, least, high):
    def one(dim, blocks):
        heights = jax.random.uniform(jax.random.fold_in(jax.random.fold_in(rng, 6), dim), (blocks,), jnp.float32, least / len(cuts), high / len(cuts))
        return jnp.repeat(jnp.exp(heights), shape[dim] // blocks).reshape((-1,) + (1,) * (len(shape) - dim - 1))

    gain = one(*cuts[0])
    for cut in cuts[1:]:
        gain = gain * one(*cut)
    return gain


def deal_out(rng, own, number, rows, count, top, reach, skew):
    order = jax.random.permutation(rng, count)
    heavy_load, usual = shares(count, rows * top, reach, skew, True), shares(count, rows * top, reach, skew, False)
    places = jnp.arange(count)

    def named(tallies, offset_by):
        used = int((tallies > 0).sum())
        fixed = max(1, used // 4)
        moved = fixed + (places - fixed + offset_by * (used - fixed)) % max(1, count - fixed)
        return jnp.zeros((count,), jnp.int32).at[order[jnp.where(places < fixed, places, moved)]].set(jnp.asarray(tallies, jnp.int32))

    tallies = jnp.where(number % 4 == 0, named(heavy_load, number // 4), named(usual, number - number // 4 - 1))
    mixed = jax.random.permutation(jax.random.fold_in(own, 3), count)
    donor, taker = mixed[0:count // 2 * 2:2], mixed[1:count // 2 * 2:2]
    room = jnp.minimum(tallies[donor] - 1, reach - tallies[taker]) // 2
    room = jnp.where((donor == order[0]) | (taker == order[0]) | (tallies[taker] == 0), 0, jnp.maximum(room, 0))
    moved = jax.random.randint(jax.random.fold_in(own, 4), (count // 2,), 0, 1 << 20) % (room + 1)
    tallies = tallies.at[donor].add(-moved).at[taker].add(moved)
    items = jnp.searchsorted(jnp.cumsum(tallies), jnp.arange(rows * top), side="right").astype(jnp.int32)
    grid = items.reshape(top, rows).T
    grid = grid[jax.random.permutation(jax.random.fold_in(own, 1), rows)]
    offset_by = jax.random.randint(jax.random.fold_in(own, 2), (rows, 1), 0, top)
    return jnp.take_along_axis(grid, (jnp.arange(top)[None, :] + offset_by) % top, axis=1)


def shares(number_of, total, most, lean, full):
    weights = [(1 << 20) // math.isqrt(standing ** lean) + 1 for standing in range(1, number_of + 1)]
    largest = most if full else min(most, max(-(-total // number_of), total * weights[0] // sum(weights)))
    least = 1 if total - largest >= number_of - 1 else 0
    counts, surplus = [largest] + [least] * (number_of - 1), total - largest - least * (number_of - 1)
    while surplus > 0:
        free = [i for i in range(1, number_of) if counts[i] < largest] or [i for i in range(1, number_of) if counts[i] < most]
        pool, left = sum([weights[i] for i in free]), surplus
        for i in free:
            addition = min(most - counts[i], max(1, left * weights[i] // pool), surplus)
            counts[i] = counts[i] + addition
            surplus = surplus - addition
    return np.array(counts)


def gaussian(key, shape, deviation, limit, cuts=(), held_as=jnp.bfloat16):
    drawn = deviation * jax.random.normal(key, shape, jnp.float32)
    if cuts:
        drawn = drawn * steps_of(key, shape, cuts, -0.22, 0.18)
    return jnp.clip(drawn, -limit, limit).astype(held_as)


def heavy_noise(own_key, extent, deviation, reach, shards, heavy, held_as=jnp.bfloat16):
    array = deviation * jax.random.normal(own_key, extent, jnp.float32)
    if shards:
        array = array * steps_of(own_key, extent, shards, -0.22, 0.18)
    return jnp.clip(raised(array, jax.random.fold_in(own_key, 3), *heavy), -reach, reach).astype(held_as)


def setup_inputs(seed: int = 0) -> dict:
    seeds = jax.random.split(jax.random.key(seed), 15)
    layer_input = gaussian(seeds[0], (SERIES_ENTRIES, D), 1.0, 6.0, ((0, 64), (1, 4)))
    cotangent = heavy_noise(seeds[1], (SERIES_ENTRIES, D), 1.0, 16.0, ((0, 64), (1, 4)), (0, 1, 64, 4.0))
    routes_keys = jax.random.split(jax.random.fold_in(seeds[2], 1), SERIES_ENTRIES // TOK_DEV)
    routes_turns = jax.random.permutation(jax.random.fold_in(seeds[2], 3), SERIES_ENTRIES // TOK_DEV)
    routes = jax.vmap(lambda own, number: deal_out(jax.random.fold_in(seeds[2], 2), own, number, TOK_DEV, EXPERTS, TOPK, CAP, 1))(routes_keys, routes_turns).reshape((SERIES_ENTRIES, TOPK))
    route_weight = jnp.clip(0.1 + 0.5 * jax.random.uniform(seeds[3], (SERIES_ENTRIES, TOPK), jnp.float32) ** steps_of(seeds[3], (SERIES_ENTRIES, TOPK), ((0, 64),), -0.2, 0.2), 0.1, 0.6)
    gate_weight = gaussian(seeds[4], (EXPERTS, D, EXP_HIDDEN), D ** -0.5, 0.125, ((0, 64), (2, 4)))
    up_weight = gaussian(seeds[5], (EXPERTS, D, EXP_HIDDEN), D ** -0.5, 0.125, ((0, 64), (2, 4)))
    down_weight = gaussian(seeds[6], (EXPERTS, EXP_HIDDEN, D), EXP_HIDDEN ** -0.5, 0.1875, ((0, 64), (1, 4)))
    heads_value = gaussian(seeds[7], (SERIES_ENTRIES, SSD_W), 1.0, 6.0, ((0, 64), (1, 4)))
    output_gate = gaussian(seeds[8], (SERIES_ENTRIES, SSD_W), 1.5, 8.0, ((0, 64), (1, 4)))
    mixer_saved = gaussian(seeds[9], (SERIES_ENTRIES, SSD_W), 1.0, 6.0, ((0, 64), (1, 4)))
    proj_weight = gaussian(seeds[10], (D, SSD_W), SSD_W ** -0.5, 0.125, ((1, 4),))
    state_write = gaussian(seeds[11], (SERIES_ENTRIES, GROUPS * STATE), 0.08, 0.5, ((0, 64), (1, 4)))
    state_read = gaussian(seeds[12], (SERIES_ENTRIES, GROUPS * STATE), 0.08, 0.5, ((0, 64), (1, 4)))
    decay_rate = draw_decay_rate(jax.random.fold_in(seeds[14], 71), 0)
    return dict(layer_input=layer_input, cotangent=cotangent, routes=routes, route_weight=route_weight, gate_weight=gate_weight, up_weight=up_weight, down_weight=down_weight, heads_value=heads_value, output_gate=output_gate, mixer_saved=mixer_saved, proj_weight=proj_weight, state_write=state_write, state_read=state_read, decay_rate=decay_rate)


maximal_value = lax.Precision.HIGHEST


def silu_parts(value):
    sigma = jax.nn.sigmoid(value)
    return value * sigma, sigma * (1.0 + value * (1.0 - sigma))


def slot_index(flat_routes):
    onehot = (flat_routes[:, None] == jnp.arange(EXPERTS, dtype=jnp.int32)[None, :]).astype(jnp.int32)
    before = jnp.cumsum(onehot, axis=0, dtype=jnp.int32) - onehot
    ranks = jnp.sum(before * onehot, axis=1, dtype=jnp.int32)
    return (flat_routes * CAP + ranks).astype(jnp.int32)


def block_sums(block):
    value_vectors, step_deltas, write_vectors, read_vectors, rates = block
    repeat = BLENDER_CHANNEL // GROUPS
    cumul = jnp.cumsum(rates, axis=0)
    total = cumul[-1]
    to_end = jnp.exp(cumul - total)
    to_start = jnp.exp(-cumul)
    write_heads = jnp.repeat(write_vectors, repeat, axis=1)
    read_heads = jnp.repeat(read_vectors, repeat, axis=1)
    write_end = jnp.einsum('shn,shp->hnp', write_heads * to_end[:, :, None], value_vectors, precision=maximal_value)
    read_end = jnp.einsum('shn,shp->hnp', read_heads * to_end[:, :, None], step_deltas, precision=maximal_value)
    write_start = jnp.einsum('shn,shp->hnp', write_heads * to_start[:, :, None], value_vectors, precision=maximal_value)
    read_start = jnp.einsum('shn,shp->hnp', read_heads * to_start[:, :, None], step_deltas, precision=maximal_value)
    return total, write_end, read_end, write_start, read_start


def block_grads(item):
    value_vectors, step_deltas, write_vectors, read_vectors, rates, write_low, read_low, write_high, read_high = item
    repeat = BLENDER_CHANNEL // GROUPS
    length = value_vectors.shape[0]
    cumul = jnp.cumsum(rates, axis=0)
    to_end = jnp.exp(cumul - cumul[-1])
    to_start = jnp.exp(-cumul)
    write_heads = jnp.repeat(write_vectors, repeat, axis=1)
    read_heads = jnp.repeat(read_vectors, repeat, axis=1)
    mixing_kernel = jnp.exp(-jnp.abs(cumul.T[:, :, None] - cumul.T[:, None, :]))
    common_part = jnp.repeat(jnp.einsum('tgn,sgn->gts', read_vectors, write_vectors, precision=maximal_value), repeat, axis=0)
    match_scores = jnp.einsum('thp,shp->hts', step_deltas, value_vectors, precision=maximal_value)
    weighted_values = mixing_kernel * match_scores
    value_g = jnp.einsum('hts,thp->shp', mixing_kernel * common_part, step_deltas, precision=maximal_value)
    write_g = jnp.einsum('hts,thn->shn', weighted_values, read_heads, precision=maximal_value)
    read_g = jnp.einsum('hts,shn->thn', weighted_values, write_heads, precision=maximal_value)
    value_g = value_g + jnp.einsum('hnp,thn->thp', read_low, write_heads, precision=maximal_value) * to_start[:, :, None]
    value_g = value_g + jnp.einsum('hnp,thn->thp', read_high, write_heads, precision=maximal_value) * to_end[:, :, None]
    write_g = write_g + jnp.einsum('hnp,thp->thn', read_low, value_vectors * to_start[:, :, None], precision=maximal_value)
    write_g = write_g + jnp.einsum('hnp,thp->thn', read_high, value_vectors * to_end[:, :, None], precision=maximal_value)
    read_g = read_g + jnp.einsum('hnp,thp->thn', write_low, step_deltas * to_start[:, :, None], precision=maximal_value)
    read_g = read_g + jnp.einsum('hnp,thp->thn', write_high, step_deltas * to_end[:, :, None], precision=maximal_value)
    write_g = write_g.reshape(length, GROUPS, repeat, STATE).sum(axis=2)
    read_g = read_g.reshape(length, GROUPS, repeat, STATE).sum(axis=2)
    return value_g, write_g, read_g


def reference(layer_input, cotangent, routes, route_weight, gate_weight, up_weight, down_weight,
              heads_value, output_gate, mixer_saved, proj_weight, state_write, state_read, decay_rate):
    flat = routes.reshape(N_SP, TOK_DEV * TOPK)
    slots = jax.vmap(slot_index)(flat)
    owners = jnp.arange(TOK_DEV * TOPK, dtype=jnp.int32) // TOPK
    offsets = (jnp.arange(N_SP, dtype=jnp.int32) * TOK_DEV)[:, None]

    def slot_tokens(slot_row, offset_row):
        return jnp.full((EXPERTS * CAP,), SERIES_ENTRIES, jnp.int32).at[slot_row].set(owners + offset_row)

    def slot_weights(slot_row, weight_row):
        return jnp.zeros((EXPERTS * CAP,), jnp.float32).at[slot_row].set(weight_row)

    token_table = jax.vmap(slot_tokens)(slots, offsets)
    weight_table = jax.vmap(slot_weights)(slots, route_weight.reshape(N_SP, TOK_DEV * TOPK))
    token_table = token_table.reshape(N_SP, EXPERTS, CAP).transpose(1, 0, 2).reshape(EXPERTS, N_SP * CAP)
    weight_table = weight_table.reshape(N_SP, EXPERTS, CAP).transpose(1, 0, 2).reshape(EXPERTS, N_SP * CAP)
    inputs_pad = jnp.concatenate([layer_input, jnp.zeros((1, D), layer_input.dtype)], axis=0)
    cotangent_pad = jnp.concatenate([cotangent, jnp.zeros((1, D), cotangent.dtype)], axis=0)
    width = EXP_HIDDEN // N_TP

    def expert_step(item):
        rows, weights, gate_one, up_one, down_one = item
        inputs = inputs_pad[rows]
        sent = (cotangent_pad[rows].astype(jnp.float32) * weights[:, None]).astype(jnp.bfloat16)
        pre_gate = jnp.dot(inputs, gate_one, preferred_element_type=jnp.float32)
        pre_up = jnp.dot(inputs, up_one, preferred_element_type=jnp.float32)
        active, slope = silu_parts(pre_gate)
        hidden = (active * pre_up).astype(jnp.bfloat16)
        hidden_grad = jnp.dot(sent, down_one.T, preferred_element_type=jnp.float32)
        gate_delta = (hidden_grad * pre_up * slope).astype(jnp.bfloat16)
        up_delta = (hidden_grad * active).astype(jnp.bfloat16)
        down_g = jnp.dot(hidden.T, sent, preferred_element_type=jnp.float32).astype(jnp.bfloat16)
        gate_g = jnp.dot(inputs.T, gate_delta, preferred_element_type=jnp.float32).astype(jnp.bfloat16)
        up_g = jnp.dot(inputs.T, up_delta, preferred_element_type=jnp.float32).astype(jnp.bfloat16)
        parts = jnp.einsum('rjk,djk->jrd', gate_delta.reshape(-1, N_TP, width).astype(jnp.float32),
                           gate_one.reshape(D, N_TP, width).astype(jnp.float32))
        parts = parts + jnp.einsum('rjk,djk->jrd', up_delta.reshape(-1, N_TP, width).astype(jnp.float32),
                                   up_one.reshape(D, N_TP, width).astype(jnp.float32))
        rounded = lax.optimization_barrier(parts.astype(jnp.bfloat16)).astype(jnp.float32)
        returned = jnp.sum(rounded, axis=0).astype(jnp.bfloat16)
        return gate_g, up_g, down_g, returned

    gate_grad, up_grad, down_grad, returned = lax.map(
        expert_step, (token_table, weight_table, gate_weight, up_weight, down_weight))
    expert_of = slots // CAP
    rank_of = slots % CAP
    sources = jnp.arange(N_SP, dtype=jnp.int32)[:, None]
    position = (expert_of * (N_SP * CAP) + sources * CAP + rank_of).astype(jnp.int32).reshape(-1)
    moe_grad = returned.reshape(-1, D)[position].astype(jnp.float32).reshape(SERIES_ENTRIES, TOPK, D).sum(axis=1)
    layer_grad = (cotangent.astype(jnp.float32) + moe_grad).astype(jnp.bfloat16)

    out_delta = jnp.dot(layer_grad, proj_weight, preferred_element_type=jnp.float32).astype(jnp.bfloat16)
    active_gate, slope_gate = silu_parts(output_gate.astype(jnp.float32))
    saved = mixer_saved.astype(jnp.float32)
    gated = (saved * active_gate).astype(jnp.bfloat16)
    proj_grad = jnp.dot(layer_grad.T, gated, preferred_element_type=jnp.float32)
    outgate_grad = (out_delta.astype(jnp.float32) * saved * slope_gate).astype(jnp.bfloat16)
    mixer_delta = out_delta.astype(jnp.float32) * active_gate

    blk = math.gcd(TOK_DEV, 256)
    count = SERIES_ENTRIES // blk
    value_vectors = heads_value.astype(jnp.float32).reshape(count, blk, BLENDER_CHANNEL, HEAD_DIM)
    step_deltas = mixer_delta.reshape(count, blk, BLENDER_CHANNEL, HEAD_DIM)
    write_vectors = state_write.astype(jnp.float32).reshape(count, blk, GROUPS, STATE)
    read_vectors = state_read.astype(jnp.float32).reshape(count, blk, GROUPS, STATE)
    rates = decay_rate.astype(jnp.float32).reshape(count, blk, BLENDER_CHANNEL)
    totals, write_end, read_end, write_start, read_start = lax.map(block_sums, (value_vectors, step_deltas, write_vectors, read_vectors, rates))
    zero_state = jnp.zeros((BLENDER_CHANNEL, STATE, HEAD_DIM), jnp.float32)

    def carry_on(state, item):
        total, write_part, read_part = item
        fade = jnp.exp(-total)[:, None, None]
        return (fade * state[0] + write_part, fade * state[1] + read_part), state

    _, (write_low, read_low) = lax.scan(carry_on, (zero_state, zero_state), (totals, write_end, read_end))
    _, (write_high, read_high) = lax.scan(carry_on, (zero_state, zero_state), (totals, write_start, read_start), reverse=True)
    value_g, write_g, read_g = lax.map(block_grads, (value_vectors, step_deltas, write_vectors, read_vectors, rates,
                                                     write_low, read_low, write_high, read_high))
    return (gate_grad, up_grad, down_grad, proj_grad,
            value_g.reshape(SERIES_ENTRIES, SSD_W).astype(jnp.bfloat16),
            write_g.reshape(SERIES_ENTRIES, GROUPS * STATE).astype(jnp.bfloat16),
            read_g.reshape(SERIES_ENTRIES, GROUPS * STATE).astype(jnp.bfloat16),
            outgate_grad)
```

```python
import jax
import jax.numpy as jnp
from jax import lax
from jax.experimental import pallas as pl
from jax.experimental.pallas import tpu as pltpu
from jax.sharding import Mesh
from jax.sharding import PartitionSpec as P

SP = ("sp_0", "sp_1", "sp_2")
NZ, NX, NC, NY = 8, 4, 2, 4
NSP = NZ * NX * NC
PLANE = NX * NC
T = 128
W = 512
HEADS = 8
CAP = 6
BF = jnp.bfloat16
F32 = jnp.float32
ORDER = (0, 1, 7, 2, 6, 3, 5, 4)
MESH_ID = pl.DeviceIdType.MESH
HIGH = lax.Precision.HIGHEST


def dot(a, b, ca=1, cb=0, precision=None):
    return lax.dot_general(
        a, b, (((ca,), (cb,)), ((), ())), preferred_element_type=F32, precision=precision
    )


def iota(shape, dim):
    return lax.broadcasted_iota(jnp.int32, shape, dim)


def body(
    li_h, cot_h, rt_v, rw_v, gw_h, uw_h, dw_h, hv_h, og_h, ms_h, pw_h, sw_h, sr_h, dr_v,
    gg_o, ug_o, dg_o, pg_o, vg_o, wg_o, rg_o, og_o,
    *scratch,
):
    (
        li, cot, gu, dw, hv, og, ms, pw, sw, sr, sx, gy, xm, cm, acc_gu, acc_h, gud, hid, ps,
        own, hl, hr, mrg, nl, nr, ret, rr, comb, lg, od, dl, sstw, sstr, stw, strd, low, high,
        outw, outr, wsw, wsr, fsend, frecv, vfs, vfi, dfs, dfi, fts, lst, lker, vint, lt, rtm,
        ga, pgs, zr, pgown, ow_gu, ow_d, ow_p, ow_v, ow_w, ow_r, ow_o, ld_sem, o_sem, self_sem,
        d_send, d_recv, y_send, yl_recv, yr_recv, yo_recv, rs_send, rs_recv, ret_send, ret_recv,
        lg_send, lg_recv, st_send, st_recv, ga_send, ga_recv, rt_send, rt_recv, z_send, z_recv,

    ) = scratch
    z = lax.axis_index("sp_0")
    x = lax.axis_index("sp_1")
    c = lax.axis_index("sp_2")
    y = lax.axis_index("tp")
    plane = x * NC + c
    me = z * PLANE + plane

    def ahead(dz, p):
        return (
            lax.rem(z + dz, NZ),
            lax.rem(x + p // NC, NX),
            lax.rem(c + p % NC, NC),
        )

    def behind(dz, p):
        return (
            lax.rem(z + NZ - dz, NZ),
            lax.rem(x + NX - p // NC, NX),
            lax.rem(c + p % NC, NC),
        )

    right = (z, x, c, lax.rem(y + 1, NY))
    left = (z, x, c, lax.rem(y + NY - 1, NY))
    opposite = (z, x, c, lax.rem(y + 2, NY))

    def remote(src, dst, ss, rs, dev):
        pltpu.make_async_remote_copy(
            src_ref=src, dst_ref=dst, send_sem=ss, recv_sem=rs, device_id=dev,
            device_id_type=MESH_ID,
        ).start()

    def local(src, dst, sem):
        pltpu.make_async_copy(src, dst, sem).start()

    def wait(ref, sem):
        pltpu.make_async_copy(ref, ref, sem).wait()

    def to_all(send):
        for p in range(1, PLANE):
            send(0, p)

        def step(n, _):
            odd = lax.rem(n, 2)
            dz = odd * ((n + 1) // 2) + (1 - odd) * (NZ - n // 2)
            for p in range(PLANE):
                send(dz, p)
            return 0

        lax.fori_loop(1, NZ, step, 0)

    loads = (
        (li_h, li), (cot_h, cot), (hv_h, hv), (sw_h, sw), (sr_h, sr), (og_h, og), (ms_h, ms),
        (gw_h.at[0], gu.at[:, pl.ds(0, 256)]), (uw_h.at[0], gu.at[:, pl.ds(256, 256)]),
        (dw_h.at[0], dw), (pw_h, pw),
    )
    for n, (a, b) in enumerate(loads):
        local(a, b, ld_sem.at[n])

    def loaded(n):
        wait(loads[n][1], ld_sem.at[n])

    bar = pltpu.get_barrier_semaphore()

    def greet(dev):
        pl.semaphore_signal(bar, inc=1, device_id=dev, device_id_type=MESH_ID)

    to_all(lambda dz, p: greet(ahead(dz, p) + (y,)))
    greet(right)
    greet(left)
    greet(opposite)

    ci = iota((512, T), 0)
    r8 = lax.rem(ci, 8)
    blk = ci // 8
    e = (
        lax.rem(z + blk // PLANE, NZ) * PLANE
        + lax.rem(x + lax.rem(blk // NC, NX), NX) * NC
        + lax.rem(c + lax.rem(blk, NC), NC)
    )
    r0 = jnp.broadcast_to(rt_v[0:1, :], (512, T))
    r1 = jnp.broadcast_to(rt_v[1:2, :], (512, T))
    hit = (r0 == e) | (r1 == e)
    upper = (iota((T, T), 0) < iota((T, T), 1)).astype(F32).astype(BF)
    hitf = jnp.where(hit, 1.0, 0.0)
    rank = dot(hitf.astype(BF), upper).astype(jnp.int32)
    wsel = jnp.where(
        r0 == e, jnp.broadcast_to(rw_v[0:1, :], (512, T)), jnp.broadcast_to(rw_v[1:2, :], (512, T))
    )
    base = hit & (rank == r8) & (r8 < CAP)
    basef = jnp.where(base, 1.0, 0.0)
    extra = [
        jnp.where(hit & (rank == 2 * k + r8 - CAP) & (r8 >= CAP), 1.0, 0.0) for k in range(3)
    ]
    loaded(0)
    loaded(1)
    for k in range(3):
        pick = jnp.concatenate([basef.astype(BF), extra[k].astype(BF)], axis=1)
        rows = jnp.concatenate(
            [
                jnp.concatenate([li[:, 128 * k : 128 * k + 128], cot[:, 128 * k : 128 * k + 128]], axis=1),
                jnp.concatenate([li[:, 384:512], cot[:, 384:512]], axis=1),
            ],
            axis=0,
        )
        got = dot(pick, rows)
        weight = jnp.sum((basef + extra[k]) * wsel, axis=1, keepdims=True)
        sx.at[k].reshape(512, T)[...] = got[:, :128].astype(BF)
        sx.at[3 + k].reshape(512, T)[...] = (got[:, 128:] * weight).astype(BF)

    comb[0] = basef.T.astype(BF)
    for k in range(3):
        comb[1 + k] = extra[k].T.astype(BF)

    pl.semaphore_wait(bar, NSP - 1 + 3)

    def send_x(dz, p):
        j = dz * PLANE + p
        remote(sx.at[:, j], gy.at[0, :, j], d_send, d_recv.at[dz], ahead(dz, p) + (y,))

    local(sx.at[:, 0], gy.at[0, :, 0], self_sem.at[0])
    to_all(send_x)

    loaded(2)
    loaded(3)
    loaded(4)
    upto = (iota((T, T), 0) <= iota((T, T), 1)).astype(F32)
    cum = dot(dr_v[...], upto, precision=HIGH)
    tot = cum[:, 127:128]
    te = jnp.exp(cum - tot)
    ts = jnp.exp(-cum)
    stacked = jnp.concatenate([te, ts, cum, jnp.zeros((T - 24, T), F32)], axis=0)
    tr = stacked.T
    half = iota((T, T), 1) < 64
    for h in range(HEADS):
        fsend[h] = jnp.broadcast_to(jnp.exp(-tot[h : h + 1, :]), (1, T))
        te_c = jnp.broadcast_to(tr[:, h : h + 1], (T, T))
        ts_c = jnp.broadcast_to(tr[:, 8 + h : 9 + h], (T, T))
        fts[h] = jnp.where(half, ts_c, te_c)
        cc = jnp.broadcast_to(tr[:, 16 + h : 17 + h], (T, T))
        cr = jnp.broadcast_to(cum[h : h + 1, :], (T, T))
        lker[h] = jnp.exp(-jnp.abs(cc - cr))

    def doubled(v, h):
        other = pltpu.roll(v, 64, 1)
        return jnp.where(half, v, other) if h % 2 == 0 else jnp.where(half, other, v)

    def sides(chunk_of, first, second):
        for h in range(HEADS):
            v = doubled(chunk_of(h // 2), h)
            f = fts[h]
            second[h] = (v * f).astype(BF)
            first[h] = (v * pltpu.roll(f, 64, 1)).astype(BF)

    sides(lambda k: hv[:, 128 * k : 128 * k + 128].astype(F32), vfs, vfi)

    def states(vectors_t, first, dst):
        for h in range(0, HEADS, 2):
            s = dot(vectors_t, jnp.concatenate([first[h], first[h + 1]], axis=1))
            dst[pl.ds(8 * h, 8)] = s[:, :T].astype(BF).reshape(8, 16, T)
            dst[pl.ds(8 * h + 8, 8)] = s[:, T:].astype(BF).reshape(8, 16, T)

    swt = sw[...].astype(F32).T.astype(BF)
    states(swt, vfs, sstw)

    def send_state(src, dst, n):
        def go(dz, p):
            zz, xx, cc = ahead(dz, p)
            j = dz * PLANE + p
            remote(src.at[zz * PLANE + xx * NC + cc], dst.at[j], st_send.at[n], st_recv.at[n], (zz, xx, cc, y))

        local(src.at[me], dst.at[0], self_sem.at[1 + n])
        to_all(go)

    def send_fade(dz, p):
        zz, xx, cc = ahead(dz, p)
        j = dz * PLANE + p
        remote(fsend.at[zz], frecv.at[j], st_send.at[4], st_recv.at[4], (zz, xx, cc, y))

    local(fsend.at[z], frecv.at[0], self_sem.at[5])
    to_all(send_fade)
    send_state(sstw, stw, 0)

    loaded(5)
    loaded(6)
    ogf = og[...].astype(F32)
    sig = jax.nn.sigmoid(ogf)
    ga[0] = (ms[...].astype(F32) * (ogf * sig)).astype(BF)
    for p in range(1, PLANE):
        remote(ga.at[0], ga.at[p], ga_send, ga_recv, ahead(0, p) + (y,))

    def chunk(d, dz):
        return gy.at[d, :, pl.ds(PLANE * dz, PLANE)]

    def forward(n):
        dz = ORDER[n]
        if n % 2 == 0:
            wait(chunk(1, dz), yl_recv.at[n])
            remote(chunk(1, dz), chunk(2, dz), y_send, yo_recv.at[n], right)
        else:
            wait(chunk(3, dz), yr_recv.at[n])
            remote(chunk(3, dz), chunk(2, dz), y_send, yo_recv.at[n], left)

    for n, dz in enumerate(ORDER):
        if dz == 0:
            wait(gy.at[0, :, pl.ds(1, PLANE - 1)], d_recv.at[0])
            wait(gy.at[0, :, 0], self_sem.at[0])
        else:
            wait(chunk(0, dz), d_recv.at[dz])
        remote(chunk(0, dz), chunk(1, dz), y_send, yl_recv.at[n], right)
        remote(chunk(0, dz), chunk(3, dz), y_send, yr_recv.at[n], left)
        if n >= 1:
            forward(n - 1)

    r3 = iota((64, 8, T), 1)

    def assemble(d, first, dst):
        last = None
        for k in range(3):
            dst[:, pl.ds(512 * d + 128 * k, 128)] = gy.at[d, first + k].reshape(512, T)[...]
            moved = pltpu.roll(gy[d, first + k].astype(F32), 2 * k + 2, 1)
            last = moved if k == 0 else jnp.where(r3 // 2 == k, moved, last)
        dst[:, pl.ds(512 * d + 384, 128)] = last.reshape(512, T).astype(BF)

    def rows_of(d):
        return pl.multiple_of(lax.rem(y + NY - d, NY) * 512, 512)

    def expert_in(d, start):
        assemble(d, 0, xm)
        assemble(d, 3, cm)
        off = rows_of(d)

        def step(m, _):
            rows = pl.ds(pl.multiple_of(m * 256, 256), 256)
            a = dot(xm[rows, pl.ds(512 * d, 512)], gu[pl.ds(off, 512), :])
            b = dot(cm[rows, pl.ds(512 * d, 512)], dw[:, pl.ds(off, 512)], 1, 1)
            if start:
                acc_gu[rows, :] = a
                acc_h[rows, :] = b
            else:
                acc_gu[rows, :] += a
                acc_h[rows, :] += b
            return 0

        lax.fori_loop(0, 2, step, 0)

    loaded(7)
    loaded(8)
    loaded(9)
    forward(7)
    expert_in(0, True)
    for n in range(8):
        if n % 2 == 1:
            wait(chunk(1, ORDER[n]), yl_recv.at[n])
    expert_in(1, False)
    for n in range(8):
        if n % 2 == 0:
            wait(chunk(3, ORDER[n]), yr_recv.at[n])
    expert_in(3, False)
    for n in range(8):
        wait(chunk(2, ORDER[n]), yo_recv.at[n])
    expert_in(2, False)

    def middle(m, _):
        rows = pl.ds(pl.multiple_of(m * 64, 64), 64)
        keep = lax.rem(iota((64, 256), 0), 8) < CAP
        g = acc_gu[rows, pl.ds(0, 256)]
        u = acc_gu[rows, pl.ds(256, 256)]
        hg = acc_h[rows, :]
        s = jax.nn.sigmoid(g)
        act = g * s
        slope = s * (1.0 + g * (1.0 - s))
        hid[rows, :] = jnp.where(keep, act * u, 0.0).astype(BF)
        gud[rows, pl.ds(0, 256)] = jnp.where(keep, hg * u * slope, 0.0).astype(BF)
        gud[rows, pl.ds(256, 256)] = jnp.where(keep, hg * act, 0.0).astype(BF)
        return 0

    lax.fori_loop(0, 8, middle, 0)

    def packed(d, put):
        off = rows_of(d)

        def step(m, _):
            rows = pl.ds(pl.multiple_of(m * 128, 128), 128)
            a = dot(gud[rows, :], gu[pl.ds(off, 512), :], 1, 1)
            tail = a[:, 384:512].reshape(16, 8, T)
            rr3 = iota((16, 8, T), 1)
            for k in range(3):
                main = a[:, 128 * k : 128 * k + 128].reshape(16, 8, T)
                put(k, m, jnp.where(rr3 < CAP, main, pltpu.roll(tail, 6 - 2 * k, 1)))
            return 0

        lax.fori_loop(0, 4, step, 0)

    def put_send(d):
        def put(k, m, v):
            ps.at[d - 1, k].reshape(512, T)[pl.ds(pl.multiple_of(m * 128, 128), 128), :] = v.reshape(
                128, T
            ).astype(BF)

        return put

    def put_own(k, m, v):
        own[k, pl.ds(pl.multiple_of(m * 128, 128), 128), :] = v.reshape(128, T)

    lo = pl.ds(0, 32)
    hi = pl.ds(32, 32)
    packed(2, put_send(2))
    remote(ps.at[1, :, lo], hl, rs_send, rs_recv.at[0], right)
    remote(ps.at[1, :, hi], hr, rs_send, rs_recv.at[1], left)
    packed(3, put_send(3))
    remote(ps.at[2, :, hi], nl.at[:, hi], rs_send, rs_recv.at[2], right)
    packed(1, put_send(1))
    remote(ps.at[0, :, lo], nr.at[:, lo], rs_send, rs_recv.at[3], left)

    def merge(n, a, b):
        for k in range(3):
            mrg[n, k] = (a[k].astype(F32) + b[k].astype(F32)).astype(BF)

    wait(hl, rs_recv.at[0])
    merge(0, ps.at[2, :, lo], hl)
    remote(mrg.at[0], nl.at[:, lo], rs_send, rs_recv.at[4], right)
    wait(hr, rs_recv.at[1])
    merge(1, ps.at[0, :, hi], hr)
    remote(mrg.at[1], nr.at[:, hi], rs_send, rs_recv.at[5], left)
    packed(0, put_own)

    def scan(b, out):
        def at(i):
            return (
                lax.rem(z + NZ - i // PLANE, NZ) * PLANE
                + lax.rem(x + NX - lax.rem(i // NC, NX), NX) * NC
                + lax.rem(c + lax.rem(i, NC), NC)
            )

        def step(n, carry):
            s, t = carry
            jf = at(n)
            jb = at(NSP - 1 - n)
            low[jf] = s
            s = s * frecv[jf] + b[jf].astype(F32)
            high[jb] = t
            t = t * frecv[jb] + b[jb].astype(F32)
            return s, t

        zero = jnp.zeros((16, T), F32)
        lax.fori_loop(0, NSP, step, (zero, zero))

        def join(n, _):
            pos = pl.ds(n * 8, 8)
            out[pos] = jnp.where(iota((8, 16, T), 2) < 64, low[pos], high[pos]).astype(BF)
            return 0

        lax.fori_loop(0, 8, join, 0)

    def states_back(out, dst, n):
        def go(dz, p):
            zz, xx, cc = behind(dz, p)
            j = dz * PLANE + p
            remote(out.at[j], dst.at[me], st_send.at[n], st_recv.at[n], (zz, xx, cc, y))

        local(out.at[0], dst.at[me], self_sem.at[1 + n])
        to_all(go)

    def got_states(ref, n):
        wait(ref.at[pl.ds(1, NSP - 1)], st_recv.at[n])
        wait(ref.at[0], self_sem.at[1 + n])

    wait(frecv.at[pl.ds(1, NSP - 1)], st_recv.at[4])
    wait(frecv.at[0], self_sem.at[5])
    got_states(stw, 0)
    scan(stw, outw)

    wait(nl.at[:, hi], rs_recv.at[2])
    wait(nr.at[:, lo], rs_recv.at[3])
    wait(nl.at[:, lo], rs_recv.at[4])
    wait(nr.at[:, hi], rs_recv.at[5])
    for k in range(3):
        ret[k] = (
            own[k].reshape(64, 8, T) + nl[k].astype(F32) + nr[k].astype(F32)
        ).astype(BF)

    def send_back(dz, p):
        j = dz * PLANE + p
        remote(ret.at[:, j], rr.at[:, j], ret_send, ret_recv, behind(dz, p) + (y,))

    local(ret.at[:, 0], rr.at[:, 0], self_sem.at[6])
    to_all(send_back)
    states_back(outw, wsw, 1)

    def weight_grad(n, _):
        cols = pl.ds(pl.multiple_of(n * 256, 256), 256)
        src = pl.multiple_of(lax.rem(y + NY - n // 2, NY) * 512 + lax.rem(n, 2) * 256, 256)
        ow_gu[pl.ds(src, 256), :] = dot(xm[:, cols], gud[...], 0, 0).astype(BF)
        ow_d[:, pl.ds(src, 256)] = dot(hid[...], cm[:, cols], 0, 0).astype(BF)
        return 0

    lax.fori_loop(0, 8, weight_grad, 0)
    local(ow_gu.at[:, pl.ds(0, 256)], gg_o.at[0], o_sem.at[0])
    local(ow_gu.at[:, pl.ds(256, 256)], ug_o.at[0], o_sem.at[1])
    local(ow_d, dg_o.at[0], o_sem.at[2])

    common_t = dot(sw[...], sr[...], 1, 1)
    for h in range(HEADS):
        lst[h] = (lker[h] * common_t).astype(BF)

    wait(rr.at[:, pl.ds(1, NSP - 1)], ret_recv)
    wait(rr.at[:, 0], self_sem.at[6])
    tail = None
    for k in range(3):
        both = jnp.concatenate([comb[0], comb[1 + k]], axis=0)
        v = dot(both, rr.at[k].reshape(512, T)[...])
        lg[0, :, 128 * k : 128 * k + 128] = (
            cot[:, 128 * k : 128 * k + 128].astype(F32) + v[:T]
        ).astype(BF)
        tail = v[T:] if k == 0 else tail + v[T:]
    lg[0, :, 384:512] = (cot[:, 384:512].astype(F32) + tail).astype(BF)
    remote(lg.at[0], lg.at[1], lg_send, lg_recv.at[0], right)
    remote(lg.at[0], lg.at[3], lg_send, lg_recv.at[1], left)
    loaded(10)

    def out_part(d):
        v = dot(lg[d], pw[pl.ds(rows_of(d), 512), :])
        if d == 0:
            od[...] = v
        else:
            od[...] += v

    def transposed(d):
        for q in range(4):
            blkt = lg[d, :, 128 * q : 128 * q + 128].astype(F32).T.astype(BF)
            zz = lax.rem(y + NY - d, NY) * 2 + q // 2
            lt[zz, pl.ds(4 * (q % 2), 4)] = blkt.reshape(4, 32, T)

    out_part(0)
    wait(lg.at[1], lg_recv.at[0])
    remote(lg.at[1, pl.ds(0, 64)], lg.at[2, pl.ds(0, 64)], lg_send, lg_recv.at[2], right)
    wait(lg.at[3], lg_recv.at[1])
    remote(lg.at[3, pl.ds(64, 64)], lg.at[2, pl.ds(64, 64)], lg_send, lg_recv.at[3], left)
    out_part(1)
    out_part(3)
    transposed(0)
    transposed(1)
    transposed(3)
    wait(lg.at[2, pl.ds(0, 64)], lg_recv.at[2])
    wait(lg.at[2, pl.ds(64, 64)], lg_recv.at[3])
    out_part(2)
    odf = od[...].astype(BF).astype(F32)
    ogf = og[...].astype(F32)
    sig = jax.nn.sigmoid(ogf)
    delta = odf * (ogf * sig)
    od[...] = delta
    dl[...] = delta.astype(BF)

    sides(lambda k: od[:, 128 * k : 128 * k + 128], dfs, dfi)
    srt = sr[...].astype(F32).T.astype(BF)
    states(srt, dfs, sstr)
    send_state(sstr, strd, 2)
    transposed(2)
    for p in range(1, PLANE):
        zz, xx, cc = ahead(0, p)
        remote(
            lt.at[:, xx * NC + cc], rtm.at[:, :, pl.ds(T * p, T)], rt_send, rt_recv, (zz, xx, cc, y)
        )
    local(lt.at[:, plane], rtm.at[:, :, pl.ds(0, T)], self_sem.at[7])
    ow_o[...] = (odf * ms[...].astype(F32) * (sig * (1.0 + ogf * (1.0 - sig)))).astype(BF)
    local(ow_o, og_o, o_sem.at[7])

    wsum = None
    for h in range(HEADS):
        cols = slice(128 * (h // 2), 128 * (h // 2) + 128)
        mine = half if h % 2 == 0 else ~half
        dm = jnp.where(mine, od[:, cols], 0.0).astype(BF)
        part = lker[h] * dot(dm, hv[:, cols], 1, 1)
        wsum = part if h == 0 else wsum + part
    rgrad = dot(wsum.astype(BF), sw[...])
    wgrad = dot(wsum.T.astype(BF), sr[...])
    for k in range(HEADS // 2):
        cols = slice(128 * k, 128 * k + 128)
        a = dot(lst[2 * k], dl[:, cols])
        b = dot(lst[2 * k + 1], dl[:, cols])
        vint[:, cols] = jnp.where(half, a, b)
    got_states(wsw, 1)
    for h in range(HEADS):
        rgrad = rgrad + dot(dfi[h], wsw[pl.ds(8 * h, 8)].reshape(T, T), 1, 1)
    ow_r[...] = rgrad.astype(BF)
    local(ow_r, rg_o, o_sem.at[6])

    got_states(strd, 2)
    scan(strd, outr)
    states_back(outr, wsr, 3)

    wait(ga.at[pl.ds(1, PLANE - 1)], ga_recv)
    wait(rtm.at[:, :, pl.ds(T, T * (PLANE - 1))], rt_recv)
    wait(rtm.at[:, :, pl.ds(0, T)], self_sem.at[7])
    pg = dot(rtm[...].reshape(256, 1024), ga[...].reshape(1024, W))
    pgown[...] = pg.reshape(8, 32, W)
    pgs[...] = pg.reshape(8, 32, W).astype(BF)
    for dz in (1, 7, 2, 6, 3, 5, 4):
        zz = lax.rem(z + dz, NZ)
        remote(pgs.at[zz], zr.at[dz], z_send, z_recv, (zz, x, c, y))

    got_states(wsr, 3)
    for k in range(HEADS // 2):
        cols = slice(128 * k, 128 * k + 128)
        u = []
        for h in (2 * k, 2 * k + 1):
            state = wsr[pl.ds(8 * h, 8)].reshape(T, T)
            p = dot(sw[...], state) * fts[h]
            u.append(p + pltpu.roll(p, 64, 1))
            wgrad = wgrad + dot(vfi[h], state, 1, 1)
        ow_v[:, cols] = (vint[:, cols] + jnp.where(half, u[0], u[1])).astype(BF)
    ow_w[...] = wgrad.astype(BF)
    local(ow_v, vg_o, o_sem.at[4])
    local(ow_w, wg_o, o_sem.at[5])

    wait(zr.at[pl.ds(1, NZ - 1)], z_recv)
    total = pgown[z]
    for dz in range(1, NZ):
        total = total + zr[dz].astype(F32)
    ow_p[...] = total
    local(ow_p, pg_o, o_sem.at[3])

    wait(sx.at[:, pl.ds(1, NSP - 1)], d_send)
    wait(gy.at[pl.ds(1, 3)], y_send)
    wait(ps, rs_send)
    wait(ret.at[:, pl.ds(1, NSP - 1)], ret_send)
    wait(lg.at[pl.ds(0, 3)], lg_send)
    for n in range(4):
        wait(stw.at[pl.ds(1, NSP - 1)], st_send.at[n])
    wait(frecv.at[pl.ds(1, NSP - 1)], st_send.at[4])
    wait(ga.at[pl.ds(1, PLANE - 1)], ga_send)
    wait(rtm.at[:, :, pl.ds(T, T * (PLANE - 1))], rt_send)
    wait(zr.at[pl.ds(1, NZ - 1)], z_send)
    stores = (
        (ow_gu.at[:, pl.ds(0, 256)], gg_o.at[0]), (ow_gu.at[:, pl.ds(256, 256)], ug_o.at[0]),
        (ow_d, dg_o.at[0]), (ow_p, pg_o), (ow_v, vg_o), (ow_w, wg_o), (ow_r, rg_o), (ow_o, og_o),
    )
    for n, (a, b) in enumerate(stores):
        pltpu.make_async_copy(a, b, o_sem.at[n]).wait()


def bf(*shape):
    return pltpu.VMEM(shape, BF)


def fl(*shape):
    return pltpu.VMEM(shape, F32)


def sem(n):
    return pltpu.SemaphoreType.DMA((n,))


SCRATCH = (
    bf(T, W),
    bf(T, W),
    bf(2048, 512),
    bf(256, 2048),
    bf(T, W),
    bf(T, W),
    bf(T, W),
    bf(2048, 512),
    bf(T, T),
    bf(T, T),
    bf(6, 64, 8, T),
    bf(4, 6, 64, 8, T),
    bf(512, 2048),
    bf(512, 2048),
    fl(512, 512),
    fl(512, 256),
    bf(512, 512),
    bf(512, 256),
    bf(3, 3, 64, 8, T),
    fl(3, 512, T),
    bf(3, 32, 8, T),
    bf(3, 32, 8, T),
    bf(2, 3, 32, 8, T),
    bf(3, 64, 8, T),
    bf(3, 64, 8, T),
    bf(3, 64, 8, T),
    bf(3, 64, 8, T),
    bf(4, T, 512),
    bf(4, T, W),
    fl(T, W),
    bf(T, W),
    bf(64, 16, T),
    bf(64, 16, T),
    bf(64, 16, T),
    bf(64, 16, T),
    fl(64, 16, T),
    fl(64, 16, T),
    bf(64, 16, T),
    bf(64, 16, T),
    bf(64, 16, T),
    bf(64, 16, T),
    fl(8, 1, T),
    fl(64, 1, T),
    bf(8, T, T),
    bf(8, T, T),
    bf(8, T, T),
    bf(8, T, T),
    fl(8, T, T),
    bf(8, T, T),
    fl(8, T, T),
    fl(T, W),
    bf(8, 8, 32, T),
    bf(8, 32, 1024),
    bf(8, T, W),
    bf(8, 32, W),
    bf(8, 32, W),
    fl(8, 32, W),
    bf(2048, 512),
    bf(256, 2048),
    fl(32, W),
    bf(T, W),
    bf(T, T),
    bf(T, T),
    bf(T, W),
    sem(11),
    sem(8),
    sem(9),
    pltpu.SemaphoreType.DMA,
    sem(8),
    pltpu.SemaphoreType.DMA,
    sem(8),
    sem(8),
    sem(8),
    pltpu.SemaphoreType.DMA,
    sem(6),
    pltpu.SemaphoreType.DMA,
    pltpu.SemaphoreType.DMA,
    pltpu.SemaphoreType.DMA,
    sem(4),
    sem(5),
    sem(5),
    pltpu.SemaphoreType.DMA,
    pltpu.SemaphoreType.DMA,
    pltpu.SemaphoreType.DMA,
    pltpu.SemaphoreType.DMA,
    pltpu.SemaphoreType.DMA,
    pltpu.SemaphoreType.DMA,
)


def on_device(
    layer_input, cotangent, routes, route_weight, gate_weight, up_weight, down_weight, heads_value,
    output_gate, mixer_saved, proj_weight, state_write, state_read, decay_rate,
):
    hbm = pl.BlockSpec(memory_space=pl.ANY)
    vmem = pl.BlockSpec(memory_space=pltpu.VMEM)
    shape = jax.ShapeDtypeStruct
    return pl.pallas_call(
        body,
        name="layer_backward",
        out_shape=(
            shape((1, 2048, 256), BF), shape((1, 2048, 256), BF), shape((1, 256, 2048), BF),
            shape((32, W), F32), shape((T, W), BF), shape((T, T), BF), shape((T, T), BF),
            shape((T, W), BF),
        ),
        in_specs=[hbm, hbm, vmem, vmem] + [hbm] * 9 + [vmem],
        out_specs=tuple([hbm] * 8),
        scratch_shapes=SCRATCH,
        compiler_params=pltpu.CompilerParams(
            collective_id=0, has_side_effects=True, vmem_limit_bytes=60 * 1024 * 1024
        ),
    )(
        layer_input, cotangent, routes.T, route_weight.T, gate_weight, up_weight, down_weight,
        heads_value, output_gate, mixer_saved, proj_weight, state_write, state_read, decay_rate.T,
    )


def solution(mesh):
    split = Mesh(mesh.devices.reshape(NZ, NX, NC, mesh.shape["tp"]), SP + ("tp",))
    rows, cut = P(SP, None), P(SP, "tp")
    return jax.shard_map(
        on_device,
        mesh=split,
        in_specs=(
            cut, cut, rows, rows, P(SP, None, "tp"), P(SP, None, "tp"), P(SP, "tp", None), cut, cut,
            cut, P(None, "tp"), cut, cut, cut,
        ),
        out_specs=(
            P(SP, None, "tp"), P(SP, None, "tp"), P(SP, "tp", None), cut, cut, cut, cut, cut,
        ),
        check_vma=False,
    )
```

```python
import jax
import jax.numpy as jnp
from jax import lax
from jax.experimental import pallas as pl
from jax.experimental.pallas import tpu as pltpu
from jax.sharding import Mesh
from jax.sharding import PartitionSpec as P

SP = ("sp_0", "sp_1", "sp_2")
NZ, NX, NC, NY = 8, 4, 2, 4
NSP = NZ * NX * NC
PLANE = NX * NC
T = 128
W = 512
HEADS = 8
CAP = 6
BF = jnp.bfloat16
F32 = jnp.float32
ORDER = (0, 1, 7, 2, 6, 3, 5, 4)
GROUPS = 2
GC = NZ // GROUPS
GJ = GC * PLANE
GR = GJ * 8
MESH_ID = pl.DeviceIdType.MESH
HIGH = lax.Precision.HIGHEST


def dot(a, b, ca=1, cb=0, precision=None):
    return lax.dot_general(
        a, b, (((ca,), (cb,)), ((), ())), preferred_element_type=F32, precision=precision
    )


def iota(shape, dim):
    return lax.broadcasted_iota(jnp.int32, shape, dim)


def body(
    li_h, cot_h, rt_v, rw_v, gw_h, uw_h, dw_h, hv_h, og_h, ms_h, pw_h, sw_h, sr_h, dr_v,
    gg_o, ug_o, dg_o, pg_o, vg_o, wg_o, rg_o, og_o,
    *scratch,
):
    (
        li, cot, gu, dw, hv, og, ms, pw, sw, sr, sx, gy, xm, cm, acc_gu, acc_h, gud, hid, ps,
        own, hl, hr, mrg, nl, nr, ret, rr, comb, lg, od, dl, sstw, sstr, stw, strd, low, high,
        outw, outr, wsw, wsr, fsend, frecv, vfs, vfi, dfs, dfi, fts, lst, lker, vint, lt, rtm,
        ga, pgs, zr, pgown, ld_sem, self_sem,
        d_send, d_recv, y_send, yl_recv, yr_recv, yo_recv, rs_send, rs_recv, ret_send, ret_recv,
        lg_send, lg_recv, st_send, st_recv, ga_send, ga_recv, rt_send, rt_recv, z_send, z_recv,

    ) = scratch
    z = lax.axis_index("sp_0")
    x = lax.axis_index("sp_1")
    c = lax.axis_index("sp_2")
    y = lax.axis_index("tp")
    plane = x * NC + c
    me = z * PLANE + plane

    def ahead(dz, p):
        return (
            lax.rem(z + dz, NZ),
            lax.rem(x + p // NC, NX),
            lax.rem(c + p % NC, NC),
        )

    def behind(dz, p):
        return (
            lax.rem(z + NZ - dz, NZ),
            lax.rem(x + NX - p // NC, NX),
            lax.rem(c + p % NC, NC),
        )

    right = (z, x, c, lax.rem(y + 1, NY))
    left = (z, x, c, lax.rem(y + NY - 1, NY))
    opposite = (z, x, c, lax.rem(y + 2, NY))

    def remote(src, dst, ss, rs, dev):
        pltpu.make_async_remote_copy(
            src_ref=src, dst_ref=dst, send_sem=ss, recv_sem=rs, device_id=dev,
            device_id_type=MESH_ID,
        ).start()

    def local(src, dst, sem):
        pltpu.make_async_copy(src, dst, sem).start()

    def wait(ref, sem):
        pltpu.make_async_copy(ref, ref, sem).wait()

    def dz_of(n):
        odd = lax.rem(n, 2)
        return lax.rem(odd * ((n + 1) // 2) + (1 - odd) * (NZ - n // 2), NZ)

    def n_of(dz):
        far = dz // 5
        return (1 - far) * (2 * dz - 1) + far * (16 - 2 * dz) + (NZ - dz) // NZ

    def to_all(send, first=0, last=NZ):
        if first == 0:
            for p in range(1, PLANE):
                send(0, 0, p)

        def step(n, _):
            dz = dz_of(n)
            for p in range(PLANE):
                send(n, dz, p)
            return 0

        lax.fori_loop(max(first, 1), last, step, 0)

    loads = (
        (li_h, li), (cot_h, cot), (hv_h, hv), (sw_h, sw), (sr_h, sr), (og_h, og), (ms_h, ms),
        (gw_h.at[0], gu.at[:, pl.ds(0, 256)]), (uw_h.at[0], gu.at[:, pl.ds(256, 256)]),
        (dw_h.at[0], dw), (pw_h, pw),
    )
    for n, (a, b) in enumerate(loads):
        local(a, b, ld_sem.at[n])

    def loaded(n):
        wait(loads[n][1], ld_sem.at[n])

    bar = pltpu.get_barrier_semaphore()

    def greet(dev):
        pl.semaphore_signal(bar, inc=1, device_id=dev, device_id_type=MESH_ID)

    to_all(lambda n, dz, p: greet(ahead(dz, p) + (y,)))
    greet(right)
    greet(left)
    greet(opposite)

    ci = iota((512, T), 0)
    r8 = lax.rem(ci, 8)
    blk = ci // 8
    e = (
        lax.rem(z + dz_of(blk // PLANE), NZ) * PLANE
        + lax.rem(x + lax.rem(blk // NC, NX), NX) * NC
        + lax.rem(c + lax.rem(blk, NC), NC)
    )
    r0 = jnp.broadcast_to(rt_v[0:1, :], (512, T))
    r1 = jnp.broadcast_to(rt_v[1:2, :], (512, T))
    hit = (r0 == e) | (r1 == e)
    upper = (iota((T, T), 0) < iota((T, T), 1)).astype(F32).astype(BF)
    hitf = jnp.where(hit, 1.0, 0.0)
    rank = dot(hitf.astype(BF), upper).astype(jnp.int32)
    wsel = jnp.where(
        r0 == e, jnp.broadcast_to(rw_v[0:1, :], (512, T)), jnp.broadcast_to(rw_v[1:2, :], (512, T))
    )
    base = hit & (rank == r8) & (r8 < CAP)
    basef = jnp.where(base, 1.0, 0.0)
    extra = [
        jnp.where(hit & (rank == 2 * k + r8 - CAP) & (r8 >= CAP), 1.0, 0.0) for k in range(3)
    ]
    loaded(0)
    loaded(1)
    for k in range(3):
        pick = jnp.concatenate([basef.astype(BF), extra[k].astype(BF)], axis=1)
        rows = jnp.concatenate(
            [
                jnp.concatenate([li[:, 128 * k : 128 * k + 128], cot[:, 128 * k : 128 * k + 128]], axis=1),
                jnp.concatenate([li[:, 384:512], cot[:, 384:512]], axis=1),
            ],
            axis=0,
        )
        got = dot(pick, rows)
        weight = jnp.sum((basef + extra[k]) * wsel, axis=1, keepdims=True)
        sx.at[k].reshape(512, T)[...] = got[:, :128].astype(BF)
        sx.at[3 + k].reshape(512, T)[...] = (got[:, 128:] * weight).astype(BF)

    comb[0] = basef.T.astype(BF)
    for k in range(3):
        comb[1 + k] = extra[k].T.astype(BF)

    loaded(2)
    loaded(3)
    loaded(4)
    upto = (iota((T, T), 0) <= iota((T, T), 1)).astype(F32)
    cum = dot(dr_v[...], upto, precision=HIGH)
    tot = cum[:, 127:128]
    te = jnp.exp(cum - tot)
    ts = jnp.exp(-cum)
    stacked = jnp.concatenate([te, ts, cum, jnp.zeros((T - 24, T), F32)], axis=0)
    tr = stacked.T
    half = iota((T, T), 1) < 64
    for h in range(HEADS):
        fsend[h] = jnp.broadcast_to(jnp.exp(-tot[h : h + 1, :]), (1, T))
        te_c = jnp.broadcast_to(tr[:, h : h + 1], (T, T))
        ts_c = jnp.broadcast_to(tr[:, 8 + h : 9 + h], (T, T))
        fts[h] = jnp.where(half, ts_c, te_c)
        cc = jnp.broadcast_to(tr[:, 16 + h : 17 + h], (T, T))
        cr = jnp.broadcast_to(cum[h : h + 1, :], (T, T))
        lker[h] = jnp.exp(-jnp.abs(cc - cr))

    def doubled(v, h):
        other = pltpu.roll(v, 64, 1)
        return jnp.where(half, v, other) if h % 2 == 0 else jnp.where(half, other, v)

    def sides(chunk_of, first, second):
        for h in range(HEADS):
            v = doubled(chunk_of(h // 2), h)
            f = fts[h]
            second[h] = (v * f).astype(BF)
            first[h] = (v * pltpu.roll(f, 64, 1)).astype(BF)

    sides(lambda k: hv[:, 128 * k : 128 * k + 128].astype(F32), vfs, vfi)

    def states(vectors_t, first, dst):
        for h in range(0, HEADS, 2):
            s = dot(vectors_t, jnp.concatenate([first[h], first[h + 1]], axis=1))
            dst[pl.ds(8 * h, 8)] = s[:, :T].astype(BF).reshape(8, 16, T)
            dst[pl.ds(8 * h + 8, 8)] = s[:, T:].astype(BF).reshape(8, 16, T)

    swt = sw[...].astype(F32).T.astype(BF)
    states(swt, vfs, sstw)

    def send_state(src, dst, n):
        def go(n_, dz, p):
            zz, xx, cc = ahead(dz, p)
            j = n_ * PLANE + p
            remote(src.at[zz * PLANE + xx * NC + cc], dst.at[j], st_send.at[n], st_recv.at[n], (zz, xx, cc, y))

        local(src.at[me], dst.at[0], self_sem.at[1 + n])
        to_all(go)

    def send_fade(n, dz, p):
        zz, xx, cc = ahead(dz, p)
        j = n * PLANE + p
        remote(fsend.at[zz], frecv.at[j], st_send.at[4], st_recv.at[4], (zz, xx, cc, y))

    loaded(5)
    loaded(6)
    ogf = og[...].astype(F32)
    sig = jax.nn.sigmoid(ogf)
    ga[0] = (ms[...].astype(F32) * (ogf * sig)).astype(BF)
    pl.semaphore_wait(bar, NSP - 1 + 3)

    def send_x(n, dz, p):
        j = n * PLANE + p
        remote(sx.at[:, j], gy.at[0, :, j], d_send, d_recv.at[n], ahead(dz, p) + (y,))

    local(sx.at[:, 0], gy.at[0, :, 0], self_sem.at[0])
    to_all(send_x)

    local(fsend.at[z], frecv.at[0], self_sem.at[5])
    to_all(send_fade)
    send_state(sstw, stw, 0)

    for p in range(1, PLANE):
        remote(ga.at[0], ga.at[p], ga_send, ga_recv, ahead(0, p) + (y,))

    def chunk(d, n):
        return gy.at[d, :, pl.ds(PLANE * n, PLANE)]

    def forward(n):
        if n % 2 == 0:
            wait(chunk(1, n), yl_recv.at[n])
            remote(chunk(1, n), chunk(2, n), y_send, yo_recv.at[n], right)
        else:
            wait(chunk(3, n), yr_recv.at[n])
            remote(chunk(3, n), chunk(2, n), y_send, yo_recv.at[n], left)

    def arrived(n):
        if n == 0:
            wait(gy.at[0, :, pl.ds(1, PLANE - 1)], d_recv.at[0])
            wait(gy.at[0, :, 0], self_sem.at[0])
        else:
            wait(chunk(0, n), d_recv.at[n])
        remote(chunk(0, n), chunk(1, n), y_send, yl_recv.at[n], right)
        remote(chunk(0, n), chunk(3, n), y_send, yr_recv.at[n], left)

    def slices(g, d):
        for n in range(GC * g, GC * g + GC):
            if d == 1 and n % 2 == 1:
                wait(chunk(1, n), yl_recv.at[n])
            if d == 3 and n % 2 == 0:
                wait(chunk(3, n), yr_recv.at[n])
            if d == 2:
                wait(chunk(2, n), yo_recv.at[n])

    r3 = iota((GJ, 8, T), 1)

    def assemble(g, d, first, dst):
        last = None
        rows = pl.ds(GR * g, GR)
        js = pl.ds(GJ * g, GJ)
        for k in range(3):
            dst[rows, pl.ds(512 * d + 128 * k, 128)] = gy.at[d, first + k].reshape(512, T)[rows, :]
            moved = pltpu.roll(gy[d, first + k, js].astype(F32), 2 * k + 2, 1)
            last = moved if k == 0 else jnp.where(r3 // 2 == k, moved, last)
        dst[rows, pl.ds(512 * d + 384, 128)] = last.reshape(GR, T).astype(BF)

    def rows_of(d):
        return pl.multiple_of(lax.rem(y + NY - d, NY) * 512, 512)

    def expert_in(g, d):
        slices(g, d)
        assemble(g, d, 0, xm)
        assemble(g, d, 3, cm)
        off = rows_of(d)
        rows = pl.ds(GR * g, GR)
        a = dot(xm[rows, pl.ds(512 * d, 512)], gu[pl.ds(off, 512), :])
        b = dot(cm[rows, pl.ds(512 * d, 512)], dw[:, pl.ds(off, 512)], 1, 1)
        if d == 0:
            acc_gu[rows, :] = a
            acc_h[rows, :] = b
        else:
            acc_gu[rows, :] += a
            acc_h[rows, :] += b

    def activations(g):
        def middle(m, _):
            rows = pl.ds(pl.multiple_of(GR * g + m * 64, 64), 64)
            keep = lax.rem(iota((64, 256), 0), 8) < CAP
            gt = acc_gu[rows, pl.ds(0, 256)]
            u = acc_gu[rows, pl.ds(256, 256)]
            hg = acc_h[rows, :]
            s = jax.nn.sigmoid(gt)
            act = gt * s
            slope = s * (1.0 + gt * (1.0 - s))
            hid[rows, :] = jnp.where(keep, act * u, 0.0).astype(BF)
            gud[rows, pl.ds(0, 256)] = jnp.where(keep, hg * u * slope, 0.0).astype(BF)
            gud[rows, pl.ds(256, 256)] = jnp.where(keep, hg * act, 0.0).astype(BF)
            return 0

        lax.fori_loop(0, GR // 64, middle, 0)

    def packed(g, d, put):
        off = rows_of(d)

        def step(m, _):
            rows = pl.ds(pl.multiple_of(GR * g + m * 128, 128), 128)
            a = dot(gud[rows, :], gu[pl.ds(off, 512), :], 1, 1)
            tail = a[:, 384:512].reshape(16, 8, T)
            rr3 = iota((16, 8, T), 1)
            for k in range(3):
                main = a[:, 128 * k : 128 * k + 128].reshape(16, 8, T)
                put(k, rows, jnp.where(rr3 < CAP, main, pltpu.roll(tail, 6 - 2 * k, 1)))
            return 0

        lax.fori_loop(0, GR // 128, step, 0)

    def put_send(d):
        def put(k, rows, v):
            ps.at[d - 1, k].reshape(512, T)[rows, :] = v.reshape(128, T).astype(BF)

        return put

    def put_own(k, rows, v):
        own[k, rows, :] = v.reshape(128, T)

    HJ = GJ // 2

    def lo(g):
        return pl.ds(GJ * g, HJ)

    def hi(g):
        return pl.ds(GJ * g + HJ, HJ)

    def far_partials(g):
        packed(g, 2, put_send(2))
        remote(ps.at[1, :, lo(g)], hl.at[g], rs_send, rs_recv.at[6 * g], right)
        remote(ps.at[1, :, hi(g)], hr.at[g], rs_send, rs_recv.at[6 * g + 1], left)

    def right_partials(g):
        packed(g, 3, put_send(3))
        remote(ps.at[2, :, hi(g)], nl.at[:, hi(g)], rs_send, rs_recv.at[6 * g + 2], right)

    def left_partials(g):
        packed(g, 1, put_send(1))
        remote(ps.at[0, :, lo(g)], nr.at[:, lo(g)], rs_send, rs_recv.at[6 * g + 3], left)

    def merge(g):
        wait(hl.at[g], rs_recv.at[6 * g])
        for k in range(3):
            mrg[0, g, k] = (ps[2, k, lo(g)].astype(F32) + hl[g, k].astype(F32)).astype(BF)
        remote(mrg.at[0, g], nl.at[:, lo(g)], rs_send, rs_recv.at[6 * g + 4], right)
        wait(hr.at[g], rs_recv.at[6 * g + 1])
        for k in range(3):
            mrg[1, g, k] = (ps[0, k, hi(g)].astype(F32) + hr[g, k].astype(F32)).astype(BF)
        remote(mrg.at[1, g], nr.at[:, hi(g)], rs_send, rs_recv.at[6 * g + 5], left)

    def send_back(n, dz, p):
        j = n * PLANE + p
        remote(ret.at[:, j], rr.at[:, j], ret_send, ret_recv.at[n // GC], behind(dz, p) + (y,))

    def give_back(g):
        wait(nl.at[:, hi(g)], rs_recv.at[6 * g + 2])
        wait(nr.at[:, lo(g)], rs_recv.at[6 * g + 3])
        wait(nl.at[:, lo(g)], rs_recv.at[6 * g + 4])
        wait(nr.at[:, hi(g)], rs_recv.at[6 * g + 5])
        js = pl.ds(GJ * g, GJ)
        for k in range(3):
            ret[k, js] = (
                own[k, pl.ds(GR * g, GR)].reshape(GJ, 8, T)
                + nl[k, js].astype(F32)
                + nr[k, js].astype(F32)
            ).astype(BF)
        if g == 0:
            local(ret.at[:, 0], rr.at[:, 0], self_sem.at[6])
        to_all(send_back, GC * g, GC * g + GC)

    for n in range(4):
        arrived(n)
        if n >= 2:
            forward(n - 2)
    loaded(7)
    loaded(8)
    loaded(9)
    arrived(4)
    forward(2)
    expert_in(0, 0)
    arrived(5)
    forward(3)
    expert_in(0, 1)
    arrived(6)
    forward(4)
    expert_in(0, 3)
    arrived(7)
    forward(5)
    expert_in(0, 2)
    forward(6)
    activations(0)
    forward(7)
    far_partials(0)
    right_partials(0)
    left_partials(0)
    expert_in(1, 0)
    merge(0)
    expert_in(1, 1)
    packed(0, 0, put_own)
    expert_in(1, 3)
    expert_in(1, 2)
    activations(1)
    far_partials(1)
    right_partials(1)
    left_partials(1)
    give_back(0)
    merge(1)
    packed(1, 0, put_own)

    def scan(b, out):
        def at(i):
            return (
                n_of(lax.rem(z + NZ - i // PLANE, NZ)) * PLANE
                + lax.rem(x + NX - lax.rem(i // NC, NX), NX) * NC
                + lax.rem(c + lax.rem(i, NC), NC)
            )

        def step(n, carry):
            s, t = carry
            jf = at(n)
            jb = at(NSP - 1 - n)
            low[jf] = s
            s = s * frecv[jf] + b[jf].astype(F32)
            high[jb] = t
            t = t * frecv[jb] + b[jb].astype(F32)
            return s, t

        zero = jnp.zeros((16, T), F32)
        lax.fori_loop(0, NSP, step, (zero, zero))

        def join(n, _):
            pos = pl.ds(n * 8, 8)
            out[pos] = jnp.where(iota((8, 16, T), 2) < 64, low[pos], high[pos]).astype(BF)
            return 0

        lax.fori_loop(0, 8, join, 0)

    def states_back(out, dst, n):
        def go(n_, dz, p):
            zz, xx, cc = behind(dz, p)
            j = n_ * PLANE + p
            remote(out.at[j], dst.at[me], st_send.at[n], st_recv.at[n], (zz, xx, cc, y))

        local(out.at[0], dst.at[me], self_sem.at[1 + n])
        to_all(go)

    def got_states(ref, n):
        wait(ref.at[pl.ds(1, NSP - 1)], st_recv.at[n])
        wait(ref.at[0], self_sem.at[1 + n])

    wait(frecv.at[pl.ds(1, NSP - 1)], st_recv.at[4])
    wait(frecv.at[0], self_sem.at[5])
    got_states(stw, 0)
    scan(stw, outw)

    give_back(1)
    states_back(outw, wsw, 1)

    def weight_grad(n, _):
        cols = pl.ds(pl.multiple_of(n * 256, 256), 256)
        src = pl.multiple_of(lax.rem(y + NY - n // 2, NY) * 512 + lax.rem(n, 2) * 256, 256)
        both = dot(xm[:, cols], gud[...], 0, 0).astype(BF)
        gg_o[0, pl.ds(src, 256), :] = both[:, :256]
        ug_o[0, pl.ds(src, 256), :] = both[:, 256:]
        dg_o[0, :, pl.ds(src, 256)] = dot(hid[...], cm[:, cols], 0, 0).astype(BF)
        return 0

    lax.fori_loop(0, 8, weight_grad, 0)
    common_t = dot(sw[...], sr[...], 1, 1)
    for h in range(HEADS):
        lst[h] = (lker[h] * common_t).astype(BF)

    moe = None
    for g in range(GROUPS):
        if g == 0:
            wait(rr.at[:, pl.ds(1, GJ - 1)], ret_recv.at[0])
            wait(rr.at[:, 0], self_sem.at[6])
        else:
            wait(rr.at[:, pl.ds(GJ * g, GJ)], ret_recv.at[g])
        cs = slice(GR * g, GR * g + GR)
        parts = []
        tail = None
        for k in range(3):
            both = jnp.concatenate([comb[0, :, cs], comb[1 + k, :, cs]], axis=0)
            v = dot(both, rr.at[k].reshape(512, T)[pl.ds(GR * g, GR), :])
            parts.append(v[:T])
            tail = v[T:] if k == 0 else tail + v[T:]
        parts.append(tail)
        moe = parts if g == 0 else [m + q for m, q in zip(moe, parts)]
    for k in range(4):
        lg[0, :, 128 * k : 128 * k + 128] = (
            cot[:, 128 * k : 128 * k + 128].astype(F32) + moe[k]
        ).astype(BF)
    remote(lg.at[0], lg.at[1], lg_send, lg_recv.at[0], right)
    remote(lg.at[0], lg.at[3], lg_send, lg_recv.at[1], left)
    loaded(10)

    def out_part(d):
        v = dot(lg[d], pw[pl.ds(rows_of(d), 512), :])
        if d == 0:
            od[...] = v
        else:
            od[...] += v

    def transposed(d):
        for q in range(4):
            blkt = lg[d, :, 128 * q : 128 * q + 128].astype(F32).T.astype(BF)
            zz = lax.rem(y + NY - d, NY) * 2 + q // 2
            lt[zz, pl.ds(4 * (q % 2), 4)] = blkt.reshape(4, 32, T)

    out_part(0)
    wait(lg.at[1], lg_recv.at[0])
    remote(lg.at[1, pl.ds(0, 64)], lg.at[2, pl.ds(0, 64)], lg_send, lg_recv.at[2], right)
    wait(lg.at[3], lg_recv.at[1])
    remote(lg.at[3, pl.ds(64, 64)], lg.at[2, pl.ds(64, 64)], lg_send, lg_recv.at[3], left)
    out_part(1)
    out_part(3)
    transposed(0)
    transposed(1)
    transposed(3)
    wait(lg.at[2, pl.ds(0, 64)], lg_recv.at[2])
    wait(lg.at[2, pl.ds(64, 64)], lg_recv.at[3])
    out_part(2)
    odf = od[...].astype(BF).astype(F32)
    ogf = og[...].astype(F32)
    sig = jax.nn.sigmoid(ogf)
    delta = odf * (ogf * sig)
    od[...] = delta
    dl[...] = delta.astype(BF)

    sides(lambda k: od[:, 128 * k : 128 * k + 128], dfs, dfi)
    srt = sr[...].astype(F32).T.astype(BF)
    states(srt, dfs, sstr)
    send_state(sstr, strd, 2)
    transposed(2)
    for p in range(1, PLANE):
        zz, xx, cc = ahead(0, p)
        remote(
            lt.at[:, xx * NC + cc], rtm.at[:, :, pl.ds(T * p, T)], rt_send, rt_recv, (zz, xx, cc, y)
        )
    local(lt.at[:, plane], rtm.at[:, :, pl.ds(0, T)], self_sem.at[7])
    og_o[...] = (odf * ms[...].astype(F32) * (sig * (1.0 + ogf * (1.0 - sig)))).astype(BF)

    wsum = None
    for h in range(HEADS):
        cols = slice(128 * (h // 2), 128 * (h // 2) + 128)
        mine = half if h % 2 == 0 else ~half
        dm = jnp.where(mine, od[:, cols], 0.0).astype(BF)
        part = lker[h] * dot(dm, hv[:, cols], 1, 1)
        wsum = part if h == 0 else wsum + part
    rgrad = dot(wsum.astype(BF), sw[...])
    wgrad = dot(wsum.T.astype(BF), sr[...])
    for k in range(HEADS // 2):
        cols = slice(128 * k, 128 * k + 128)
        a = dot(lst[2 * k], dl[:, cols])
        b = dot(lst[2 * k + 1], dl[:, cols])
        vint[:, cols] = jnp.where(half, a, b)
    got_states(wsw, 1)
    for h in range(HEADS):
        rgrad = rgrad + dot(dfi[h], wsw[pl.ds(8 * h, 8)].reshape(T, T), 1, 1)
    rg_o[...] = rgrad.astype(BF)

    got_states(strd, 2)
    scan(strd, outr)
    states_back(outr, wsr, 3)

    wait(ga.at[pl.ds(1, PLANE - 1)], ga_recv)
    wait(rtm.at[:, :, pl.ds(T, T * (PLANE - 1))], rt_recv)
    wait(rtm.at[:, :, pl.ds(0, T)], self_sem.at[7])
    pg = dot(rtm[...].reshape(256, 1024), ga[...].reshape(1024, W))
    pgown[...] = pg.reshape(8, 32, W)
    pgs[...] = pg.reshape(8, 32, W).astype(BF)
    for dz in (1, 7, 2, 6, 3, 5, 4):
        zz = lax.rem(z + dz, NZ)
        remote(pgs.at[zz], zr.at[dz], z_send, z_recv, (zz, x, c, y))

    got_states(wsr, 3)
    for k in range(HEADS // 2):
        cols = slice(128 * k, 128 * k + 128)
        u = []
        for h in (2 * k, 2 * k + 1):
            state = wsr[pl.ds(8 * h, 8)].reshape(T, T)
            p = dot(sw[...], state) * fts[h]
            u.append(p + pltpu.roll(p, 64, 1))
            wgrad = wgrad + dot(vfi[h], state, 1, 1)
        vg_o[:, cols] = (vint[:, cols] + jnp.where(half, u[0], u[1])).astype(BF)
    wg_o[...] = wgrad.astype(BF)

    wait(zr.at[pl.ds(1, NZ - 1)], z_recv)
    total = pgown[z]
    for dz in range(1, NZ):
        total = total + zr[dz].astype(F32)
    pg_o[...] = total

    wait(sx.at[:, pl.ds(1, NSP - 1)], d_send)
    wait(gy.at[pl.ds(1, 3)], y_send)
    wait(ps, rs_send)
    wait(ret.at[:, pl.ds(1, NSP - 1)], ret_send)
    wait(lg.at[pl.ds(0, 3)], lg_send)
    for n in range(4):
        wait(stw.at[pl.ds(1, NSP - 1)], st_send.at[n])
    wait(frecv.at[pl.ds(1, NSP - 1)], st_send.at[4])
    wait(ga.at[pl.ds(1, PLANE - 1)], ga_send)
    wait(rtm.at[:, :, pl.ds(T, T * (PLANE - 1))], rt_send)
    wait(zr.at[pl.ds(1, NZ - 1)], z_send)


def bf(*shape):
    return pltpu.VMEM(shape, BF)


def fl(*shape):
    return pltpu.VMEM(shape, F32)


def sem(n):
    return pltpu.SemaphoreType.DMA((n,))


SCRATCH = (
    bf(T, W),
    bf(T, W),
    bf(2048, 512),
    bf(256, 2048),
    bf(T, W),
    bf(T, W),
    bf(T, W),
    bf(2048, 512),
    bf(T, T),
    bf(T, T),
    bf(6, 64, 8, T),
    bf(4, 6, 64, 8, T),
    bf(512, 2048),
    bf(512, 2048),
    fl(512, 512),
    fl(512, 256),
    bf(512, 512),
    bf(512, 256),
    bf(3, 3, 64, 8, T),
    fl(3, 512, T),
    bf(GROUPS, 3, GJ // 2, 8, T),
    bf(GROUPS, 3, GJ // 2, 8, T),
    bf(2, GROUPS, 3, GJ // 2, 8, T),
    bf(3, 64, 8, T),
    bf(3, 64, 8, T),
    bf(3, 64, 8, T),
    bf(3, 64, 8, T),
    bf(4, T, 512),
    bf(4, T, W),
    fl(T, W),
    bf(T, W),
    bf(64, 16, T),
    bf(64, 16, T),
    bf(64, 16, T),
    bf(64, 16, T),
    fl(64, 16, T),
    fl(64, 16, T),
    bf(64, 16, T),
    bf(64, 16, T),
    bf(64, 16, T),
    bf(64, 16, T),
    fl(8, 1, T),
    fl(64, 1, T),
    bf(8, T, T),
    bf(8, T, T),
    bf(8, T, T),
    bf(8, T, T),
    fl(8, T, T),
    bf(8, T, T),
    fl(8, T, T),
    fl(T, W),
    bf(8, 8, 32, T),
    bf(8, 32, 1024),
    bf(8, T, W),
    bf(8, 32, W),
    bf(8, 32, W),
    fl(8, 32, W),
    sem(11),
    sem(9),
    pltpu.SemaphoreType.DMA,
    sem(8),
    pltpu.SemaphoreType.DMA,
    sem(8),
    sem(8),
    sem(8),
    pltpu.SemaphoreType.DMA,
    sem(6 * GROUPS),
    pltpu.SemaphoreType.DMA,
    sem(GROUPS),
    pltpu.SemaphoreType.DMA,
    sem(4),
    sem(5),
    sem(5),
    pltpu.SemaphoreType.DMA,
    pltpu.SemaphoreType.DMA,
    pltpu.SemaphoreType.DMA,
    pltpu.SemaphoreType.DMA,
    pltpu.SemaphoreType.DMA,
    pltpu.SemaphoreType.DMA,
)


def on_device(
    layer_input, cotangent, routes, route_weight, gate_weight, up_weight, down_weight, heads_value,
    output_gate, mixer_saved, proj_weight, state_write, state_read, decay_rate,
):
    hbm = pl.BlockSpec(memory_space=pl.ANY)
    vmem = pl.BlockSpec(memory_space=pltpu.VMEM)
    shapes = (
        ((1, 2048, 256), BF), ((1, 2048, 256), BF), ((1, 256, 2048), BF), ((32, W), F32),
        ((T, W), BF), ((T, T), BF), ((T, T), BF), ((T, W), BF),
    )
    results = pl.pallas_call(
        body,
        name="layer_backward",
        out_shape=tuple(pltpu.VMEM(s, t) for s, t in shapes),
        in_specs=[hbm, hbm, vmem, vmem] + [hbm] * 9 + [vmem],
        out_specs=tuple([vmem] * 8),
        scratch_shapes=SCRATCH,
        compiler_params=pltpu.CompilerParams(
            collective_id=0, has_side_effects=True, vmem_limit_bytes=52 * 1024 * 1024
        ),
    )(
        layer_input, cotangent, routes.T, route_weight.T, gate_weight, up_weight, down_weight,
        heads_value, output_gate, mixer_saved, proj_weight, state_write, state_read, decay_rate.T,
    )

    def store(*refs):
        sems = refs[-1]
        copies = [
            pltpu.make_async_copy(refs[n], refs[8 + n], sems.at[n]) for n in range(8)
        ]
        for copy in copies:
            copy.start()
        for copy in copies:
            copy.wait()

    return pl.pallas_call(
        store,
        name="store",
        out_shape=tuple(jax.ShapeDtypeStruct(s, t) for s, t in shapes),
        in_specs=[vmem] * 8,
        out_specs=tuple([hbm] * 8),
        scratch_shapes=[sem(8)],
        compiler_params=pltpu.CompilerParams(vmem_limit_bytes=8 * 1024 * 1024),
    )(*results)


def solution(mesh):
    split = Mesh(mesh.devices.reshape(NZ, NX, NC, mesh.shape["tp"]), SP + ("tp",))
    rows, cut = P(SP, None), P(SP, "tp")
    return jax.shard_map(
        on_device,
        mesh=split,
        in_specs=(
            cut, cut, rows, rows, P(SP, None, "tp"), P(SP, None, "tp"), P(SP, "tp", None), cut, cut,
            cut, P(None, "tp"), cut, cut, cut,
        ),
        out_specs=(
            P(SP, None, "tp"), P(SP, None, "tp"), P(SP, "tp", None), cut, cut, cut, cut, cut,
        ),
        check_vma=False,
    )
```

```python
import jax
import jax.numpy as jnp
from jax import lax
from jax.experimental import pallas as pl
from jax.experimental.pallas import tpu as pltpu
from jax.sharding import Mesh
from jax.sharding import PartitionSpec as P

SP = ("sp_0", "sp_1", "sp_2")
NZ, NX, NC, NY = 8, 4, 2, 4
NSP = NZ * NX * NC
PLANE = NX * NC
T = 128
W = 512
HEADS = 8
CAP = 6
BF = jnp.bfloat16
F32 = jnp.float32
ORDER = (0, 2, 6, 5, 3, 4, 7, 1)
PACKED = sum(d << (3 * n) for n, d in enumerate(ORDER))
PLACES = sum(n << (3 * d) for n, d in enumerate(ORDER))
GROUPS = 4
GC = NZ // GROUPS
GJ = GC * PLANE
GR = GJ * 8
MESH_ID = pl.DeviceIdType.MESH
HIGH = lax.Precision.HIGHEST


def dot(a, b, ca=1, cb=0, precision=None):
    return lax.dot_general(
        a, b, (((ca,), (cb,)), ((), ())), preferred_element_type=F32, precision=precision
    )


def iota(shape, dim):
    return lax.broadcasted_iota(jnp.int32, shape, dim)


def body(
    li_h, cot_h, rt_h, rw_h, gw_h, uw_h, dw_h, hv_h, og_h, ms_h, pw_h, sw_h, sr_h, dr_h,
    gg_o, ug_o, dg_o, pg_o, vg_o, wg_o, rg_o, og_o,
    *scratch,
):
    (
        rt_v, rw_v, dr_v, li, cot, gu, dw, hv, og, ms, pw, sw, sr, sx, gy, xm, cm, acc_gu, acc_h, gud, hid, ps,
        own, hl, hr, mrg, nl, nr, ret, rr, comb, lg, od, dl, sstw, sstr, low, inb, zs, zb, outb, fplane, fade_send, fade_recv,
        wsw, wsr, fsend, frecv, vfs, vfi, dfs, dfi, fts, lst, lker, vint, lt, rtm,
        ga, pgs, zr, pgown, ld_sem, self_sem, in_sem, out_sem,
        d_send, d_recv, y_send, yl_recv, yr_recv, yo_recv, rs_send, rs_recv, ret_send, ret_recv,
        lg_send, lg_recv, st_send, st_recv, ga_send, ga_recv, rt_send, rt_recv, z_send, z_recv,
    ) = scratch
    z = lax.axis_index("sp_0")
    x = lax.axis_index("sp_1")
    c = lax.axis_index("sp_2")
    y = lax.axis_index("tp")
    plane = x * NC + c
    me = z * PLANE + plane

    def ahead(dz, p):
        return (
            lax.rem(z + dz, NZ),
            lax.rem(x + p // NC, NX),
            lax.rem(c + p % NC, NC),
        )

    def behind(dz, p):
        return (
            lax.rem(z + NZ - dz, NZ),
            lax.rem(x + NX - p // NC, NX),
            lax.rem(c + p % NC, NC),
        )

    right = (z, x, c, lax.rem(y + 1, NY))
    left = (z, x, c, lax.rem(y + NY - 1, NY))
    opposite = (z, x, c, lax.rem(y + 2, NY))

    def remote(src, dst, ss, rs, dev):
        pltpu.make_async_remote_copy(
            src_ref=src, dst_ref=dst, send_sem=ss, recv_sem=rs, device_id=dev,
            device_id_type=MESH_ID,
        ).start()

    def local(src, dst, sem):
        pltpu.make_async_copy(src, dst, sem).start()

    def wait(ref, sem):
        pltpu.make_async_copy(ref, ref, sem).wait()

    def dz_of(n):
        return lax.shift_right_logical(jnp.int32(PACKED), 3 * n) & 7

    def n_of(dz):
        return lax.shift_right_logical(jnp.int32(PLACES), 3 * dz) & 7

    def dz_vec(n):
        out = jnp.zeros_like(n)
        for k, d in enumerate(ORDER):
            out = jnp.where(n == k, d, out)
        return out

    def to_all(send, first=0, last=NZ):
        if first == 0:
            for p in range(1, PLANE):
                send(0, 0, p)

        def step(n, _):
            dz = dz_of(n)
            for p in range(PLANE):
                send(n, dz, p)
            return 0

        lax.fori_loop(max(first, 1), last, step, 0)

    loads = (
        (li_h, li), (cot_h, cot), (hv_h, hv), (sw_h, sw), (sr_h, sr), (og_h, og), (ms_h, ms),
        (gw_h.at[0], gu.at[:, pl.ds(0, 256)]), (uw_h.at[0], gu.at[:, pl.ds(256, 256)]),
        (dw_h.at[0], dw), (pw_h, pw), (rt_h, rt_v), (rw_h, rw_v), (dr_h, dr_v),
    )
    for n in (11, 12, 13, 0, 1, 2, 3, 4, 5, 6, 7, 8, 9, 10):
        local(*loads[n], ld_sem.at[n])

    def loaded(n):
        wait(loads[n][1], ld_sem.at[n])

    bar = pltpu.get_barrier_semaphore()

    def greet(dev):
        pl.semaphore_signal(bar, inc=1, device_id=dev, device_id_type=MESH_ID)

    to_all(lambda n, dz, p: greet(ahead(dz, p) + (y,)))
    greet(right)
    greet(left)
    greet(opposite)

    loaded(11)
    loaded(12)
    loaded(13)
    ci = iota((512, T), 0)
    r8 = lax.rem(ci, 8)
    blk = ci // 8
    e = (
        lax.rem(z + dz_vec(blk // PLANE), NZ) * PLANE
        + lax.rem(x + lax.rem(blk // NC, NX), NX) * NC
        + lax.rem(c + lax.rem(blk, NC), NC)
    )
    r0 = jnp.broadcast_to(rt_v[0:1, :], (512, T))
    r1 = jnp.broadcast_to(rt_v[1:2, :], (512, T))
    hit = (r0 == e) | (r1 == e)
    upper = (iota((T, T), 0) < iota((T, T), 1)).astype(F32).astype(BF)
    hitf = jnp.where(hit, 1.0, 0.0)
    rank = dot(hitf.astype(BF), upper).astype(jnp.int32)
    wsel = jnp.where(
        r0 == e, jnp.broadcast_to(rw_v[0:1, :], (512, T)), jnp.broadcast_to(rw_v[1:2, :], (512, T))
    )
    base = hit & (rank == r8) & (r8 < CAP)
    basef = jnp.where(base, 1.0, 0.0)
    extra = [
        jnp.where(hit & (rank == 2 * k + r8 - CAP) & (r8 >= CAP), 1.0, 0.0) for k in range(3)
    ]
    loaded(0)
    loaded(1)
    for k in range(3):
        pick = jnp.concatenate([basef.astype(BF), extra[k].astype(BF)], axis=1)
        rows = jnp.concatenate(
            [
                jnp.concatenate([li[:, 128 * k : 128 * k + 128], cot[:, 128 * k : 128 * k + 128]], axis=1),
                jnp.concatenate([li[:, 384:512], cot[:, 384:512]], axis=1),
            ],
            axis=0,
        )
        got = dot(pick, rows)
        weight = jnp.sum((basef + extra[k]) * wsel, axis=1, keepdims=True)
        sx.at[k].reshape(512, T)[...] = got[:, :128].astype(BF)
        sx.at[3 + k].reshape(512, T)[...] = (got[:, 128:] * weight).astype(BF)

    comb[0] = basef.T.astype(BF)
    for k in range(3):
        comb[1 + k] = extra[k].T.astype(BF)

    loaded(2)
    loaded(3)
    loaded(4)
    upto = (iota((T, T), 0) <= iota((T, T), 1)).astype(F32)
    cum = dot(dr_v[...], upto, precision=HIGH)
    tot = cum[:, 127:128]
    te = jnp.exp(cum - tot)
    ts = jnp.exp(-cum)
    stacked = jnp.concatenate([te, ts, cum, jnp.zeros((T - 24, T), F32)], axis=0)
    tr = stacked.T
    half = iota((T, T), 1) < 64
    for h in range(HEADS):
        fsend[h] = jnp.broadcast_to(jnp.exp(-tot[h : h + 1, :]), (1, T))
        te_c = jnp.broadcast_to(tr[:, h : h + 1], (T, T))
        ts_c = jnp.broadcast_to(tr[:, 8 + h : 9 + h], (T, T))
        fts[h] = jnp.where(half, ts_c, te_c)
        cc = jnp.broadcast_to(tr[:, 16 + h : 17 + h], (T, T))
        cr = jnp.broadcast_to(cum[h : h + 1, :], (T, T))
        lker[h] = jnp.exp(-jnp.abs(cc - cr))

    def doubled(v, h):
        other = pltpu.roll(v, 64, 1)
        return jnp.where(half, v, other) if h % 2 == 0 else jnp.where(half, other, v)

    def sides(chunk_of, first, second):
        for h in range(HEADS):
            v = doubled(chunk_of(h // 2), h)
            f = fts[h]
            second[h] = (v * f).astype(BF)
            first[h] = (v * pltpu.roll(f, 64, 1)).astype(BF)

    sides(lambda k: hv[:, 128 * k : 128 * k + 128].astype(F32), vfs, vfi)

    def states(vectors_t, first, dst):
        for h in range(0, HEADS, 2):
            s = dot(vectors_t, jnp.concatenate([first[h], first[h + 1]], axis=1))
            dst[h] = s[:, :T].astype(BF)
            dst[h + 1] = s[:, T:].astype(BF)

    swt = sw[...].astype(F32).T.astype(BF)
    states(swt, vfs, sstw)

    def place(i):
        return lax.rem(x + NX - i // NC, NX) * NC + lax.rem(c + i % NC, NC)

    def rowhalf(u):
        return pl.ds(64 * u, 64)

    quarter = iota((32, T), 1) < 64

    def packed_half(v, at_left):
        other = pltpu.roll(v[:32] if not at_left else v[32:], 64, 1)
        return jnp.where(quarter, v[:32] if at_left else other, other if at_left else v[32:])

    def send_plane(src, e):
        for u in range(2):
            k = 6 * e + 3 * u
            for p in range(1, PLANE):
                zz, xx, cc = ahead(0, p)
                remote(
                    src.at[xx * NC + cc, rowhalf(u)], inb.at[e, u, p], st_send.at[k], st_recv.at[k],
                    (zz, xx, cc, y),
                )
            local(src.at[plane, rowhalf(u)], inb.at[e, u, 0], in_sem.at[2 * e + u])

    def plane_totals(e, u):
        k = 6 * e + 3 * u
        wait(inb.at[e, u, pl.ds(1, PLANE - 1)], st_recv.at[k])
        wait(inb.at[e, u, 0], in_sem.at[2 * e + u])
        up = None
        down = None
        for i in range(PLANE):
            p = place(i)
            q = place(PLANE - 1 - i)
            v = inb[e, u, p].astype(F32)
            w = inb[e, u, q].astype(F32)
            up = v if i == 0 else up * frecv[p] + v
            down = w if i == 0 else down * frecv[q] + w
        zs[e, u, 0] = packed_half(up, True).astype(BF)
        zs[e, u, 1] = packed_half(down, False).astype(BF)
        for dz in (4, 5, 3, 6, 2, 1, 7):
            zz = lax.rem(z + dz, NZ)
            remote(
                zs.at[e, u, (z + dz) // NZ], zb.at[e, u, dz], st_send.at[k + 1], st_recv.at[k + 1],
                (zz, x, c, y),
            )

    def spread(e, u, dst):
        k = 6 * e + 3 * u
        wait(zb.at[e, u, pl.ds(1, NZ - 1)], st_recv.at[k + 1])
        up = jnp.zeros((32, T), F32)
        down = jnp.zeros((32, T), F32)
        for i in range(NZ):
            dz = lax.rem(z + NZ - i, NZ)
            f = fplane[n_of(dz)]
            v = zb[e, u, dz].astype(F32)
            up = jnp.where((z - i + NZ - 1) // NZ == 1, up * f + v, up)
            r = NZ - 1 - i
            dz = lax.rem(z + NZ - r, NZ)
            f = fplane[n_of(dz)]
            v = zb[e, u, dz].astype(F32)
            down = jnp.where((r - z + NZ - 1) // NZ == 1, down * f + v, down)
        start = jnp.concatenate(
            [
                jnp.where(quarter, up, pltpu.roll(down, 64, 1)),
                jnp.where(quarter, pltpu.roll(up, 64, 1), down),
            ],
            axis=0,
        )
        cur = start
        for i in range(PLANE):
            p = place(i)
            low[p] = cur
            if i < PLANE - 1:
                cur = cur * frecv[p] + inb[e, u, p].astype(F32)
        cur = start
        for i in reversed(range(PLANE)):
            p = place(i)
            outb[e, u, p] = jnp.where(half[:64], low[p], cur).astype(BF)
            if i > 0:
                cur = cur * frecv[p] + inb[e, u, p].astype(F32)
        for p in range(1, PLANE):
            zz, xx, cc = behind(0, p)
            remote(
                outb.at[e, u, p], dst.at[plane, rowhalf(u)], st_send.at[k + 2], st_recv.at[k + 2],
                (zz, xx, cc, y),
            )
        local(outb.at[e, u, 0], dst.at[plane, rowhalf(u)], out_sem.at[2 * e + u])

    def got_states(ref, e):
        for u in range(2):
            wait(inb.at[e, u, pl.ds(1, PLANE - 1)], st_recv.at[6 * e + 3 * u + 2])
            wait(ref.at[0, rowhalf(u)], out_sem.at[2 * e + u])

    def fades_here():
        wait(frecv.at[pl.ds(1, NSP - 1)], fade_recv)
        wait(frecv.at[0], self_sem.at[5])
        for n in range(NZ):
            f = frecv[PLANE * n]
            for p in range(1, PLANE):
                f = f * frecv[PLANE * n + p]
            fplane[n] = f

    def send_fade(n, dz, p):
        zz, xx, cc = ahead(dz, p)
        j = n * PLANE + p
        remote(fsend.at[xx * NC + cc], frecv.at[j], fade_send, fade_recv, (zz, xx, cc, y))

    loaded(5)
    loaded(6)
    ogf = og[...].astype(F32)
    sig = jax.nn.sigmoid(ogf)
    ga[0] = (ms[...].astype(F32) * (ogf * sig)).astype(BF)
    pl.semaphore_wait(bar, NSP - 1 + 3)

    def send_x(n, dz, p):
        j = n * PLANE + p
        remote(sx.at[:, j], gy.at[0, :, j], d_send, d_recv.at[n], ahead(dz, p) + (y,))

    local(sx.at[:, 0], gy.at[0, :, 0], self_sem.at[0])
    to_all(send_x)

    local(fsend.at[plane], frecv.at[0], self_sem.at[5])
    for e in range(2):
        for u in range(2):
            zb[e, u, 0] = jnp.zeros((32, T), BF)
    to_all(send_fade)
    send_plane(sstw, 0)

    for p in range(1, PLANE):
        remote(ga.at[0], ga.at[p], ga_send, ga_recv, ahead(0, p) + (y,))

    def chunk(d, n):
        return gy.at[d, :, pl.ds(PLANE * n, PLANE)]

    def forward(n):
        if n % 2 == 0:
            wait(chunk(1, n), yl_recv.at[n])
            remote(chunk(1, n), chunk(2, n), y_send, yo_recv.at[n], right)
        else:
            wait(chunk(3, n), yr_recv.at[n])
            remote(chunk(3, n), chunk(2, n), y_send, yo_recv.at[n], left)

    def arrived(n):
        if n == 0:
            wait(gy.at[0, :, pl.ds(1, PLANE - 1)], d_recv.at[0])
            wait(gy.at[0, :, 0], self_sem.at[0])
        else:
            wait(chunk(0, n), d_recv.at[n])
        remote(chunk(0, n), chunk(1, n), y_send, yl_recv.at[n], right)
        remote(chunk(0, n), chunk(3, n), y_send, yr_recv.at[n], left)

    def slices(g, d):
        for n in range(GC * g, GC * g + GC):
            if d == 1 and n % 2 == 1:
                wait(chunk(1, n), yl_recv.at[n])
            if d == 3 and n % 2 == 0:
                wait(chunk(3, n), yr_recv.at[n])
            if d == 2:
                wait(chunk(2, n), yo_recv.at[n])

    r3 = iota((GJ, 8, T), 1)

    def assemble(g, d, first, dst):
        last = None
        rows = pl.ds(GR * g, GR)
        js = pl.ds(GJ * g, GJ)
        for k in range(3):
            dst[rows, pl.ds(512 * d + 128 * k, 128)] = gy.at[d, first + k].reshape(512, T)[rows, :]
            moved = pltpu.roll(gy[d, first + k, js].astype(F32), 2 * k + 2, 1)
            last = moved if k == 0 else jnp.where(r3 // 2 == k, moved, last)
        dst[rows, pl.ds(512 * d + 384, 128)] = last.reshape(GR, T).astype(BF)

    def rows_of(d):
        return pl.multiple_of(lax.rem(y + NY - d, NY) * 512, 512)

    def expert_in(g, d):
        slices(g, d)
        assemble(g, d, 0, xm)
        assemble(g, d, 3, cm)
        off = rows_of(d)
        rows = pl.ds(GR * g, GR)
        a = dot(xm[rows, pl.ds(512 * d, 512)], gu[pl.ds(off, 512), :])
        b = dot(cm[rows, pl.ds(512 * d, 512)], dw[:, pl.ds(off, 512)], 1, 1)
        if d == 0:
            acc_gu[rows, :] = a
            acc_h[rows, :] = b
        else:
            acc_gu[rows, :] += a
            acc_h[rows, :] += b

    def activations(g):
        def middle(m, _):
            rows = pl.ds(pl.multiple_of(GR * g + m * 64, 64), 64)
            keep = lax.rem(iota((64, 256), 0), 8) < CAP
            gt = acc_gu[rows, pl.ds(0, 256)]
            u = acc_gu[rows, pl.ds(256, 256)]
            hg = acc_h[rows, :]
            s = jax.nn.sigmoid(gt)
            act = gt * s
            slope = s * (1.0 + gt * (1.0 - s))
            hid[rows, :] = jnp.where(keep, act * u, 0.0).astype(BF)
            gud[rows, pl.ds(0, 256)] = jnp.where(keep, hg * u * slope, 0.0).astype(BF)
            gud[rows, pl.ds(256, 256)] = jnp.where(keep, hg * act, 0.0).astype(BF)
            return 0

        lax.fori_loop(0, GR // 64, middle, 0)

    def packed(g, d, put):
        off = rows_of(d)

        def step(m, _):
            rows = pl.ds(pl.multiple_of(GR * g + m * 128, 128), 128)
            a = dot(gud[rows, :], gu[pl.ds(off, 512), :], 1, 1)
            tail = a[:, 384:512].reshape(16, 8, T)
            rr3 = iota((16, 8, T), 1)
            for k in range(3):
                main = a[:, 128 * k : 128 * k + 128].reshape(16, 8, T)
                put(k, rows, jnp.where(rr3 < CAP, main, pltpu.roll(tail, 6 - 2 * k, 1)))
            return 0

        lax.fori_loop(0, GR // 128, step, 0)

    def put_send(d):
        def put(k, rows, v):
            ps.at[d - 1, k].reshape(512, T)[rows, :] = v.reshape(128, T).astype(BF)

        return put

    def put_own(k, rows, v):
        own[k, rows, :] = v.reshape(128, T)

    HJ = GJ // 2

    def lo(g):
        return pl.ds(GJ * g, HJ)

    def hi(g):
        return pl.ds(GJ * g + HJ, HJ)

    def far_partials(g):
        packed(g, 2, put_send(2))
        remote(ps.at[1, :, lo(g)], hl.at[g], rs_send, rs_recv.at[6 * g], right)
        remote(ps.at[1, :, hi(g)], hr.at[g], rs_send, rs_recv.at[6 * g + 1], left)

    def right_partials(g):
        packed(g, 3, put_send(3))
        remote(ps.at[2, :, hi(g)], nl.at[:, hi(g)], rs_send, rs_recv.at[6 * g + 2], right)

    def left_partials(g):
        packed(g, 1, put_send(1))
        remote(ps.at[0, :, lo(g)], nr.at[:, lo(g)], rs_send, rs_recv.at[6 * g + 3], left)

    def merge(g):
        wait(hl.at[g], rs_recv.at[6 * g])
        for k in range(3):
            mrg[0, g, k] = (ps[2, k, lo(g)].astype(F32) + hl[g, k].astype(F32)).astype(BF)
        remote(mrg.at[0, g], nl.at[:, lo(g)], rs_send, rs_recv.at[6 * g + 4], right)
        wait(hr.at[g], rs_recv.at[6 * g + 1])
        for k in range(3):
            mrg[1, g, k] = (ps[0, k, hi(g)].astype(F32) + hr[g, k].astype(F32)).astype(BF)
        remote(mrg.at[1, g], nr.at[:, hi(g)], rs_send, rs_recv.at[6 * g + 5], left)

    def send_back(n, dz, p):
        j = n * PLANE + p
        remote(ret.at[:, j], rr.at[:, j], ret_send, ret_recv.at[n // GC], behind(dz, p) + (y,))

    def give_back(g):
        wait(nl.at[:, hi(g)], rs_recv.at[6 * g + 2])
        wait(nr.at[:, lo(g)], rs_recv.at[6 * g + 3])
        wait(nl.at[:, lo(g)], rs_recv.at[6 * g + 4])
        wait(nr.at[:, hi(g)], rs_recv.at[6 * g + 5])
        js = pl.ds(GJ * g, GJ)
        for k in range(3):
            ret[k, js] = (
                own[k, pl.ds(GR * g, GR)].reshape(GJ, 8, T)
                + nl[k, js].astype(F32)
                + nr[k, js].astype(F32)
            ).astype(BF)
        if g == 0:
            local(ret.at[:, 0], rr.at[:, 0], self_sem.at[6])
        to_all(send_back, GC * g, GC * g + GC)

    def partials(g):
        activations(g)
        far_partials(g)
        right_partials(g)
        left_partials(g)

    def own_partials(g):
        packed(g, 0, put_own)

    def weight_grad(n):
        cols = pl.ds(256 * n, 256)
        src = pl.multiple_of(lax.rem(y + NY - n // 2, NY) * 512 + (n % 2) * 256, 256)
        both = dot(xm[:, cols], gud[...], 0, 0).astype(BF)
        gg_o[0, pl.ds(src, 256), :] = both[:, :256]
        ug_o[0, pl.ds(src, 256), :] = both[:, 256:]
        dg_o[0, :, pl.ds(src, 256)] = dot(hid[...], cm[:, cols], 0, 0).astype(BF)

    arrived(0)
    arrived(1)
    forward(0)
    arrived(2)
    forward(1)
    loaded(7)
    loaded(8)
    loaded(9)
    expert_in(0, 0)
    expert_in(0, 1)
    expert_in(0, 3)
    arrived(3)
    forward(2)
    expert_in(0, 2)
    partials(0)
    arrived(4)
    forward(3)
    expert_in(1, 0)
    expert_in(1, 1)
    expert_in(1, 3)
    arrived(5)
    fades_here()
    plane_totals(0, 0)
    plane_totals(0, 1)
    forward(4)
    merge(0)
    expert_in(1, 2)
    partials(1)
    own_partials(0)
    arrived(6)
    forward(5)
    arrived(7)
    spread(0, 0, wsw)
    spread(0, 1, wsw)
    forward(6)
    expert_in(2, 0)
    expert_in(2, 1)
    expert_in(2, 3)
    forward(7)
    merge(1)
    expert_in(2, 2)
    partials(2)
    own_partials(1)
    expert_in(3, 0)
    expert_in(3, 1)
    expert_in(3, 3)
    give_back(0)
    expert_in(3, 2)
    partials(3)
    own_partials(2)
    merge(2)
    own_partials(3)
    give_back(1)
    weight_grad(0)
    weight_grad(1)
    merge(3)
    weight_grad(2)
    give_back(2)
    weight_grad(3)
    give_back(3)

    for n in range(4, 6):
        weight_grad(n)
    common_t = dot(sw[...], sr[...], 1, 1)
    for h in range(HEADS):
        lst[h] = (lker[h] * common_t).astype(BF)

    moe = None
    for g in range(GROUPS):
        if g == 0:
            wait(rr.at[:, pl.ds(1, GJ - 1)], ret_recv.at[0])
            wait(rr.at[:, 0], self_sem.at[6])
        else:
            wait(rr.at[:, pl.ds(GJ * g, GJ)], ret_recv.at[g])
        cs = slice(GR * g, GR * g + GR)
        parts = []
        tail = None
        for k in range(3):
            both = jnp.concatenate([comb[0, :, cs], comb[1 + k, :, cs]], axis=0)
            v = dot(both, rr.at[k].reshape(512, T)[pl.ds(GR * g, GR), :])
            parts.append(v[:T])
            tail = v[T:] if k == 0 else tail + v[T:]
        parts.append(tail)
        moe = parts if g == 0 else [m + q for m, q in zip(moe, parts)]
    for k in range(4):
        lg[0, :, 128 * k : 128 * k + 128] = (
            cot[:, 128 * k : 128 * k + 128].astype(F32) + moe[k]
        ).astype(BF)
    first = pl.ds(0, 64)
    second = pl.ds(64, 64)
    remote(lg.at[0, first], lg.at[1, first], lg_send, lg_recv.at[0], right)
    remote(lg.at[0, second], lg.at[3, second], lg_send, lg_recv.at[1], left)
    remote(lg.at[0, second], lg.at[1, second], lg_send, lg_recv.at[2], right)
    remote(lg.at[0, first], lg.at[3, first], lg_send, lg_recv.at[3], left)
    loaded(10)

    def out_part(d):
        v = dot(lg[d], pw[pl.ds(rows_of(d), 512), :])
        if d == 0:
            od[...] = v
        else:
            od[...] += v

    def transposed(d):
        yy = lax.rem(y + NY - d, NY)
        for q in range(4):
            blkt = lg[d, :, 128 * q : 128 * q + 128].astype(F32).T.astype(BF)
            lt[yy * 2 + q // 2, pl.ds(4 * (q % 2), 4)] = blkt.reshape(4, 32, T)
        pair = pl.ds(yy * 2, 2)
        for p in range(1, PLANE):
            zz, xx, cc = ahead(0, p)
            remote(
                lt.at[pair, xx * NC + cc], rtm.at[pair, :, pl.ds(T * p, T)], rt_send, rt_recv,
                (zz, xx, cc, y),
            )

    out_part(0)
    weight_grad(6)
    weight_grad(7)
    wait(lg.at[1, first], lg_recv.at[0])
    remote(lg.at[1, first], lg.at[2, first], lg_send, lg_recv.at[4], right)
    wait(lg.at[3, second], lg_recv.at[1])
    remote(lg.at[3, second], lg.at[2, second], lg_send, lg_recv.at[5], left)
    transposed(0)
    wait(lg.at[1, second], lg_recv.at[2])
    wait(lg.at[3, first], lg_recv.at[3])
    out_part(1)
    out_part(3)
    transposed(1)
    transposed(3)
    wait(lg.at[2, first], lg_recv.at[4])
    wait(lg.at[2, second], lg_recv.at[5])
    out_part(2)
    odf = od[...].astype(BF).astype(F32)
    ogf = og[...].astype(F32)
    sig = jax.nn.sigmoid(ogf)
    delta = odf * (ogf * sig)
    od[...] = delta
    dl[...] = delta.astype(BF)

    sides(lambda k: od[:, 128 * k : 128 * k + 128], dfs, dfi)
    srt = sr[...].astype(F32).T.astype(BF)
    states(srt, dfs, sstr)
    send_plane(sstr, 1)
    transposed(2)
    local(lt.at[:, plane], rtm.at[:, :, pl.ds(0, T)], self_sem.at[7])
    og_o[...] = (odf * ms[...].astype(F32) * (sig * (1.0 + ogf * (1.0 - sig)))).astype(BF)

    wsum = None
    for h in range(HEADS):
        cols = slice(128 * (h // 2), 128 * (h // 2) + 128)
        mine = half if h % 2 == 0 else ~half
        dm = jnp.where(mine, od[:, cols], 0.0).astype(BF)
        part = lker[h] * dot(dm, hv[:, cols], 1, 1)
        wsum = part if h == 0 else wsum + part
    rgrad = dot(wsum.astype(BF), sw[...])
    wgrad = dot(wsum.T.astype(BF), sr[...])
    for k in range(HEADS // 2):
        cols = slice(128 * k, 128 * k + 128)
        a = dot(lst[2 * k], dl[:, cols])
        b = dot(lst[2 * k + 1], dl[:, cols])
        vint[:, cols] = jnp.where(half, a, b)
    plane_totals(1, 0)
    plane_totals(1, 1)
    got_states(wsw, 0)
    for h in range(HEADS):
        rgrad = rgrad + dot(dfi[h], wsw[h], 1, 1)
    rg_o[...] = rgrad.astype(BF)

    wait(ga.at[pl.ds(1, PLANE - 1)], ga_recv)
    wait(rtm.at[:, :, pl.ds(T, T * (PLANE - 1))], rt_recv)
    wait(rtm.at[:, :, pl.ds(0, T)], self_sem.at[7])
    pg = dot(rtm[...].reshape(256, 1024), ga[...].reshape(1024, W))
    pgown[...] = pg.reshape(8, 32, W)
    pgs[...] = pg.reshape(8, 32, W).astype(BF)
    for dz in (1, 7, 2, 6, 3, 5, 4):
        zz = lax.rem(z + dz, NZ)
        remote(pgs.at[zz], zr.at[dz], z_send, z_recv, (zz, x, c, y))

    spread(1, 0, wsr)
    spread(1, 1, wsr)
    got_states(wsr, 1)
    for k in range(HEADS // 2):
        cols = slice(128 * k, 128 * k + 128)
        u = []
        for h in (2 * k, 2 * k + 1):
            state = wsr[h]
            p = dot(sw[...], state) * fts[h]
            u.append(p + pltpu.roll(p, 64, 1))
            wgrad = wgrad + dot(vfi[h], state, 1, 1)
        vg_o[:, cols] = (vint[:, cols] + jnp.where(half, u[0], u[1])).astype(BF)
    wg_o[...] = wgrad.astype(BF)

    wait(zr.at[pl.ds(1, NZ - 1)], z_recv)
    total = pgown[z]
    for dz in range(1, NZ):
        total = total + zr[dz].astype(F32)
    pg_o[...] = total

    wait(sx.at[:, pl.ds(1, NSP - 1)], d_send)
    wait(gy.at[pl.ds(1, 3)], y_send)
    wait(ps, rs_send)
    wait(ret.at[:, pl.ds(1, NSP - 1)], ret_send)
    wait(lg.at[pl.ds(0, 3)], lg_send)
    for k in range(4):
        wait(inb.at[k // 2, k % 2, pl.ds(1, PLANE - 1)], st_send.at[3 * k])
        wait(zb.at[k // 2, k % 2, pl.ds(1, NZ - 1)], st_send.at[3 * k + 1])
        wait(inb.at[k // 2, k % 2, pl.ds(1, PLANE - 1)], st_send.at[3 * k + 2])
    wait(frecv.at[pl.ds(1, NSP - 1)], fade_send)
    wait(ga.at[pl.ds(1, PLANE - 1)], ga_send)
    wait(rtm.at[:, :, pl.ds(T, T * (PLANE - 1))], rt_send)
    wait(zr.at[pl.ds(1, NZ - 1)], z_send)


def bf(*shape):
    return pltpu.VMEM(shape, BF)


def fl(*shape):
    return pltpu.VMEM(shape, F32)


def sem(n):
    return pltpu.SemaphoreType.DMA((n,))


SCRATCH = (
    pltpu.VMEM((2, T), jnp.int32),
    fl(2, T),
    fl(8, T),
    bf(T, W),
    bf(T, W),
    bf(2048, 512),
    bf(256, 2048),
    bf(T, W),
    bf(T, W),
    bf(T, W),
    bf(2048, 512),
    bf(T, T),
    bf(T, T),
    bf(6, 64, 8, T),
    bf(4, 6, 64, 8, T),
    bf(512, 2048),
    bf(512, 2048),
    fl(512, 512),
    fl(512, 256),
    bf(512, 512),
    bf(512, 256),
    bf(3, 3, 64, 8, T),
    fl(3, 512, T),
    bf(GROUPS, 3, GJ // 2, 8, T),
    bf(GROUPS, 3, GJ // 2, 8, T),
    bf(2, GROUPS, 3, GJ // 2, 8, T),
    bf(3, 64, 8, T),
    bf(3, 64, 8, T),
    bf(3, 64, 8, T),
    bf(3, 64, 8, T),
    bf(4, T, 512),
    bf(4, T, W),
    fl(T, W),
    bf(T, W),
    bf(8, T, T),
    bf(8, T, T),
    fl(8, 64, T),
    bf(2, 2, 8, 64, T),
    bf(2, 2, 2, 32, T),
    bf(2, 2, 8, 32, T),
    bf(2, 2, 8, 64, T),
    fl(8, 1, T),
    pltpu.SemaphoreType.DMA,
    pltpu.SemaphoreType.DMA,
    bf(8, T, T),
    bf(8, T, T),
    fl(8, 1, T),
    fl(64, 1, T),
    bf(8, T, T),
    bf(8, T, T),
    bf(8, T, T),
    bf(8, T, T),
    fl(8, T, T),
    bf(8, T, T),
    fl(8, T, T),
    fl(T, W),
    bf(8, 8, 32, T),
    bf(8, 32, 1024),
    bf(8, T, W),
    bf(8, 32, W),
    bf(8, 32, W),
    fl(8, 32, W),
    sem(14),
    sem(9),
    sem(4),
    sem(4),
    pltpu.SemaphoreType.DMA,
    sem(8),
    pltpu.SemaphoreType.DMA,
    sem(8),
    sem(8),
    sem(8),
    pltpu.SemaphoreType.DMA,
    sem(6 * GROUPS),
    pltpu.SemaphoreType.DMA,
    sem(GROUPS),
    pltpu.SemaphoreType.DMA,
    sem(6),
    sem(12),
    sem(12),
    pltpu.SemaphoreType.DMA,
    pltpu.SemaphoreType.DMA,
    pltpu.SemaphoreType.DMA,
    pltpu.SemaphoreType.DMA,
    pltpu.SemaphoreType.DMA,
    pltpu.SemaphoreType.DMA,
)


def on_device(
    layer_input, cotangent, routes, route_weight, gate_weight, up_weight, down_weight, heads_value,
    output_gate, mixer_saved, proj_weight, state_write, state_read, decay_rate,
):
    hbm = pl.BlockSpec(memory_space=pl.ANY)
    vmem = pl.BlockSpec(memory_space=pltpu.VMEM)
    shapes = (
        ((1, 2048, 256), BF), ((1, 2048, 256), BF), ((1, 256, 2048), BF), ((32, W), F32),
        ((T, W), BF), ((T, T), BF), ((T, T), BF), ((T, W), BF),
    )
    results = pl.pallas_call(
        body,
        name="layer_backward",
        out_shape=tuple(pltpu.VMEM(s, t) for s, t in shapes),
        in_specs=[hbm] * 14,
        out_specs=tuple([vmem] * 8),
        scratch_shapes=SCRATCH,
        compiler_params=pltpu.CompilerParams(
            collective_id=0, has_side_effects=True, vmem_limit_bytes=52 * 1024 * 1024
        ),
    )(
        layer_input, cotangent, routes.T, route_weight.T, gate_weight, up_weight, down_weight,
        heads_value, output_gate, mixer_saved, proj_weight, state_write, state_read, decay_rate.T,
    )

    def store(*refs):
        sems = refs[-1]
        copies = [
            pltpu.make_async_copy(refs[n], refs[8 + n], sems.at[n]) for n in range(8)
        ]
        for copy in copies:
            copy.start()
        for copy in copies:
            copy.wait()

    return pl.pallas_call(
        store,
        name="store",
        out_shape=tuple(jax.ShapeDtypeStruct(s, t) for s, t in shapes),
        in_specs=[vmem] * 8,
        out_specs=tuple([hbm] * 8),
        scratch_shapes=[sem(8)],
        compiler_params=pltpu.CompilerParams(vmem_limit_bytes=8 * 1024 * 1024),
    )(*results)


def solution(mesh):
    split = Mesh(mesh.devices.reshape(NZ, NX, NC, mesh.shape["tp"]), SP + ("tp",))
    rows, cut = P(SP, None), P(SP, "tp")
    return jax.shard_map(
        on_device,
        mesh=split,
        in_specs=(
            cut, cut, rows, rows, P(SP, None, "tp"), P(SP, None, "tp"), P(SP, "tp", None), cut, cut,
            cut, P(None, "tp"), cut, cut, cut,
        ),
        out_specs=(
            P(SP, None, "tp"), P(SP, None, "tp"), P(SP, "tp", None), cut, cut, cut, cut, cut,
        ),
        check_vma=False,
    )
```

```python
import jax
import jax.numpy as jnp
from jax import lax
from jax.experimental import pallas as pl
from jax.experimental.pallas import tpu as pltpu
from jax.sharding import Mesh
from jax.sharding import PartitionSpec as P

SP = ("sp_0", "sp_1", "sp_2")
NZ, NX, NC, NY = 8, 4, 2, 4
NSP = NZ * NX * NC
PLANE = NX * NC
T = 128
W = 512
HEADS = 8
CAP = 6
BF = jnp.bfloat16
F32 = jnp.float32
ORDER = (0, 1, 6, 3, 5, 4, 2, 7)
PACKED = sum(d << (3 * n) for n, d in enumerate(ORDER))
PLACES = sum(n << (3 * d) for n, d in enumerate(ORDER))
GROUPS = 4
GC = NZ // GROUPS
GJ = GC * PLANE
GR = GJ * 8
MESH_ID = pl.DeviceIdType.MESH
HIGH = lax.Precision.HIGHEST


def dot(a, b, ca=1, cb=0, precision=None):
    return lax.dot_general(
        a, b, (((ca,), (cb,)), ((), ())), preferred_element_type=F32, precision=precision
    )


def iota(shape, dim):
    return lax.broadcasted_iota(jnp.int32, shape, dim)


def body(
    li_h, cot_h, rt_h, rw_h, gw_h, uw_h, dw_h, hv_h, og_h, ms_h, pw_h, sw_h, sr_h, dr_h,
    gg_o, ug_o, dg_o, pg_o, vg_o, wg_o, rg_o, og_o,
    *scratch,
):
    (
        rt_v, rw_v, dr_v, li, cot, gu, dw, hv, og, ms, pw, sw, sr, sx, gy, xm, cm, acc_gu, acc_h, gud, hid, ps,
        own, hl, hr, mrg, nl, nr, ret, rr, comb, lg, od, dl, sstw, sstr, low, inb, zs, zb, outb, fplane, fade_send, fade_recv,
        wsw, wsr, fsend, frecv, vfs, vfi, dfs, dfi, fts, lst, lker, vint, lt, rtm,
        ga, pgs, zr, pgown, ld_sem,
        d_send, d_recv, y_send, yl_recv, yr_recv, yo_recv, rs_send, rs_recv, ret_send, ret_recv,
        lg_send, lg_recv, st_send, st_recv, ga_send, ga_recv, rt_send, rt_recv, z_send, z_recv,
    ) = scratch
    z = lax.axis_index("sp_0")
    x = lax.axis_index("sp_1")
    c = lax.axis_index("sp_2")
    y = lax.axis_index("tp")
    plane = x * NC + c
    me = z * PLANE + plane

    def ahead(dz, p):
        return (
            lax.rem(z + dz, NZ),
            lax.rem(x + p // NC, NX),
            lax.rem(c + p % NC, NC),
        )

    def behind(dz, p):
        return (
            lax.rem(z + NZ - dz, NZ),
            lax.rem(x + NX - p // NC, NX),
            lax.rem(c + p % NC, NC),
        )

    right = (z, x, c, lax.rem(y + 1, NY))
    left = (z, x, c, lax.rem(y + NY - 1, NY))

    def remote(src, dst, ss, rs, dev):
        pltpu.make_async_remote_copy(
            src_ref=src, dst_ref=dst, send_sem=ss, recv_sem=rs, device_id=dev,
            device_id_type=MESH_ID,
        ).start()

    def local(src, dst, sem):
        pltpu.make_async_copy(src, dst, sem).start()

    def wait(ref, sem):
        pltpu.make_async_copy(ref, ref, sem).wait()

    def dz_of(n):
        return lax.shift_right_logical(jnp.int32(PACKED), 3 * n) & 7

    def n_of(dz):
        return lax.shift_right_logical(jnp.int32(PLACES), 3 * dz) & 7

    def dz_vec(n):
        out = jnp.zeros_like(n)
        for k, d in enumerate(ORDER):
            out = jnp.where(n == k, d, out)
        return out

    def to_all(send, first=0, last=NZ):
        if first == 0:
            for p in range(1, PLANE):
                send(0, 0, p)

        def step(n, _):
            dz = dz_of(n)
            for p in range(PLANE):
                send(n, dz, p)
            return 0

        lax.fori_loop(max(first, 1), last, step, 0)

    loads = (
        (li_h, li), (cot_h, cot), (hv_h, hv), (sw_h, sw), (sr_h, sr), (og_h, og), (ms_h, ms),
        (gw_h.at[0], gu.at[:, pl.ds(0, 256)]), (uw_h.at[0], gu.at[:, pl.ds(256, 256)]),
        (dw_h.at[0], dw), (pw_h, pw), (rt_h, rt_v), (rw_h, rw_v), (dr_h, dr_v),
    )
    for n in (11, 12, 13, 0, 1, 2, 3, 4, 5, 6, 7, 8, 9, 10):
        local(*loads[n], ld_sem.at[n])

    def loaded(n):
        wait(loads[n][1], ld_sem.at[n])

    bar = pltpu.get_barrier_semaphore()

    def greet(dev):
        pl.semaphore_signal(bar, inc=1, device_id=dev, device_id_type=MESH_ID)

    to_all(lambda n, dz, p: greet(ahead(dz, p) + (y,)))
    greet(right)
    greet(left)

    for e in range(2):
        for u in range(2):
            zb[e, u, 0] = jnp.zeros((32, T), BF)
    loaded(11)
    loaded(12)
    loaded(13)
    ci = iota((512, T), 0)
    r8 = lax.rem(ci, 8)
    blk = ci // 8
    e = (
        lax.rem(z + dz_vec(blk // PLANE), NZ) * PLANE
        + lax.rem(x + lax.rem(blk // NC, NX), NX) * NC
        + lax.rem(c + lax.rem(blk, NC), NC)
    )
    r0 = jnp.broadcast_to(rt_v[0:1, :], (512, T))
    r1 = jnp.broadcast_to(rt_v[1:2, :], (512, T))
    hit = (r0 == e) | (r1 == e)
    upper = (iota((T, T), 0) < iota((T, T), 1)).astype(F32).astype(BF)
    hitf = jnp.where(hit, 1.0, 0.0)
    rank = dot(hitf.astype(BF), upper).astype(jnp.int32)
    wsel = jnp.where(
        r0 == e, jnp.broadcast_to(rw_v[0:1, :], (512, T)), jnp.broadcast_to(rw_v[1:2, :], (512, T))
    )
    base = hit & (rank == r8) & (r8 < CAP)
    basef = jnp.where(base, 1.0, 0.0)
    extra = [
        jnp.where(hit & (rank == 2 * k + r8 - CAP) & (r8 >= CAP), 1.0, 0.0) for k in range(3)
    ]
    loaded(0)
    loaded(1)
    for k in range(3):
        pick = jnp.concatenate([basef.astype(BF), extra[k].astype(BF)], axis=1)
        rows = jnp.concatenate(
            [
                jnp.concatenate([li[:, 128 * k : 128 * k + 128], cot[:, 128 * k : 128 * k + 128]], axis=1),
                jnp.concatenate([li[:, 384:512], cot[:, 384:512]], axis=1),
            ],
            axis=0,
        )
        got = dot(pick, rows)
        weight = jnp.sum((basef + extra[k]) * wsel, axis=1, keepdims=True)
        sx.at[k].reshape(512, T)[...] = got[:, :128].astype(BF)
        sx.at[3 + k].reshape(512, T)[...] = (got[:, 128:] * weight).astype(BF)

    comb[0] = basef.T.astype(BF)
    for k in range(3):
        comb[1 + k] = extra[k].T.astype(BF)

    loaded(2)
    loaded(3)
    loaded(4)
    upto = (iota((T, T), 0) <= iota((T, T), 1)).astype(F32)
    cum = dot(dr_v[...], upto, precision=HIGH)
    tot = cum[:, 127:128]
    te = jnp.exp(cum - tot)
    ts = jnp.exp(-cum)
    stacked = jnp.concatenate([te, ts, cum, jnp.zeros((T - 24, T), F32)], axis=0)
    tr = stacked.T
    half = iota((T, T), 1) < 64
    for h in range(HEADS):
        fsend[h] = jnp.broadcast_to(jnp.exp(-tot[h : h + 1, :]), (1, T))
        te_c = jnp.broadcast_to(tr[:, h : h + 1], (T, T))
        ts_c = jnp.broadcast_to(tr[:, 8 + h : 9 + h], (T, T))
        fts[h] = jnp.where(half, ts_c, te_c)
        cc = jnp.broadcast_to(tr[:, 16 + h : 17 + h], (T, T))
        cr = jnp.broadcast_to(cum[h : h + 1, :], (T, T))
        lker[h] = jnp.exp(-jnp.abs(cc - cr))

    def doubled(v, h):
        other = pltpu.roll(v, 64, 1)
        return jnp.where(half, v, other) if h % 2 == 0 else jnp.where(half, other, v)

    def sides(chunk_of, first, second):
        for h in range(HEADS):
            v = doubled(chunk_of(h // 2), h)
            f = fts[h]
            second[h] = (v * f).astype(BF)
            first[h] = (v * pltpu.roll(f, 64, 1)).astype(BF)

    sides(lambda k: hv[:, 128 * k : 128 * k + 128].astype(F32), vfs, vfi)

    def states(vectors_t, first, dst):
        for h in range(0, HEADS, 2):
            s = dot(vectors_t, jnp.concatenate([first[h], first[h + 1]], axis=1))
            dst[h] = s[:, :T].astype(BF)
            dst[h + 1] = s[:, T:].astype(BF)

    swt = sw[...].astype(F32).T.astype(BF)
    states(swt, vfs, sstw)

    def place(i):
        return lax.rem(x + NX - i // NC, NX) * NC + lax.rem(c + i % NC, NC)

    def rowhalf(u):
        return pl.ds(64 * u, 64)

    quarter = iota((32, T), 1) < 64

    def packed_half(v, at_left):
        other = pltpu.roll(v[:32] if not at_left else v[32:], 64, 1)
        return jnp.where(quarter, v[:32] if at_left else other, other if at_left else v[32:])

    def send_plane(src, e):
        for u in range(2):
            k = 6 * e + 3 * u
            for p in range(1, PLANE):
                zz, xx, cc = ahead(0, p)
                remote(
                    src.at[xx * NC + cc, rowhalf(u)], inb.at[e, u, p], st_send.at[0], st_recv.at[k],
                    (zz, xx, cc, y),
                )
            inb[e, u, 0] = src[plane, rowhalf(u)]

    def plane_totals(e, u):
        k = 6 * e + 3 * u
        wait(inb.at[e, u, pl.ds(1, PLANE - 1)], st_recv.at[k])
        up = None
        down = None
        for i in range(PLANE):
            p = place(i)
            q = place(PLANE - 1 - i)
            v = inb[e, u, p].astype(F32)
            w = inb[e, u, q].astype(F32)
            up = v if i == 0 else up * frecv[p] + v
            down = w if i == 0 else down * frecv[q] + w
        zs[e, u, 0] = packed_half(up, True).astype(BF)
        zs[e, u, 1] = packed_half(down, False).astype(BF)
        for dz in (4, 5, 3, 6, 2, 1, 7):
            zz = lax.rem(z + dz, NZ)
            remote(
                zs.at[e, u, (z + dz) // NZ], zb.at[e, u, dz], st_send.at[1], st_recv.at[k + 1],
                (zz, x, c, y),
            )

    def spread(e, u, dst):
        k = 6 * e + 3 * u
        wait(zb.at[e, u, pl.ds(1, NZ - 1)], st_recv.at[k + 1])
        up = jnp.zeros((32, T), F32)
        down = jnp.zeros((32, T), F32)
        for i in range(NZ):
            dz = lax.rem(z + NZ - i, NZ)
            f = fplane[n_of(dz)]
            v = zb[e, u, dz].astype(F32)
            up = jnp.where((z - i + NZ - 1) // NZ == 1, up * f + v, up)
            r = NZ - 1 - i
            dz = lax.rem(z + NZ - r, NZ)
            f = fplane[n_of(dz)]
            v = zb[e, u, dz].astype(F32)
            down = jnp.where((r - z + NZ - 1) // NZ == 1, down * f + v, down)
        start = jnp.concatenate(
            [
                jnp.where(quarter, up, pltpu.roll(down, 64, 1)),
                jnp.where(quarter, pltpu.roll(up, 64, 1), down),
            ],
            axis=0,
        )
        cur = start
        for i in range(PLANE):
            p = place(i)
            low[p] = cur
            if i < PLANE - 1:
                cur = cur * frecv[p] + inb[e, u, p].astype(F32)
        cur = start
        for i in reversed(range(PLANE)):
            p = place(i)
            outb[e, u, p] = jnp.where(half[:64], low[p], cur).astype(BF)
            if i > 0:
                cur = cur * frecv[p] + inb[e, u, p].astype(F32)
        for p in range(1, PLANE):
            zz, xx, cc = behind(0, p)
            remote(
                outb.at[e, u, p], dst.at[plane, rowhalf(u)], st_send.at[2], st_recv.at[k + 2],
                (zz, xx, cc, y),
            )
        dst[plane, rowhalf(u)] = outb[e, u, 0]

    def got_states(ref, e):
        for u in range(2):
            wait(inb.at[e, u, pl.ds(1, PLANE - 1)], st_recv.at[6 * e + 3 * u + 2])

    def fades_here():
        wait(frecv.at[pl.ds(1, NSP - 1)], fade_recv)
        for n in range(NZ):
            f = frecv[PLANE * n]
            for p in range(1, PLANE):
                f = f * frecv[PLANE * n + p]
            fplane[n] = f

    def send_fade(n, dz, p):
        zz, xx, cc = ahead(dz, p)
        j = n * PLANE + p
        remote(fsend.at[xx * NC + cc], frecv.at[j], fade_send, fade_recv, (zz, xx, cc, y))

    loaded(5)
    loaded(6)
    ogf = og[...].astype(F32)
    sig = jax.nn.sigmoid(ogf)
    ga[0] = (ms[...].astype(F32) * (ogf * sig)).astype(BF)
    pl.semaphore_wait(bar, NSP - 1 + 2)

    def send_x(n, dz, p):
        j = n * PLANE + p
        remote(sx.at[:, j], gy.at[0, :, j], d_send, d_recv.at[n], ahead(dz, p) + (y,))

    gy[0, :, 0] = sx[:, 0]
    to_all(send_x)

    def chunk(d, n):
        return gy.at[d, :, pl.ds(PLANE * n, PLANE)]

    def forward(n):
        if n % 2 == 0:
            wait(chunk(1, n), yl_recv.at[n])
            remote(chunk(1, n), chunk(2, n), y_send, yo_recv.at[n // GC], right)
        else:
            wait(chunk(3, n), yr_recv.at[n])
            remote(chunk(3, n), chunk(2, n), y_send, yo_recv.at[n // GC], left)

    def arrived(n):
        if n == 0:
            wait(gy.at[0, :, pl.ds(1, PLANE - 1)], d_recv.at[0])
        else:
            wait(chunk(0, n), d_recv.at[n])
        remote(chunk(0, n), chunk(1, n), y_send, yl_recv.at[n], right)
        remote(chunk(0, n), chunk(3, n), y_send, yr_recv.at[n], left)

    def slices(g, d):
        for n in range(GC * g, GC * g + GC):
            if d == 1 and n % 2 == 1:
                wait(chunk(1, n), yl_recv.at[n])
            if d == 3 and n % 2 == 0:
                wait(chunk(3, n), yr_recv.at[n])
        if d == 2:
            wait(gy.at[2, :, pl.ds(GJ * g, GJ)], yo_recv.at[g])

    r3 = iota((GJ, 8, T), 1)

    def assemble(g, d, first, dst):
        last = None
        rows = pl.ds(GR * g, GR)
        js = pl.ds(GJ * g, GJ)
        for k in range(3):
            dst[rows, pl.ds(512 * d + 128 * k, 128)] = gy.at[d, first + k].reshape(512, T)[rows, :]
            moved = pltpu.roll(gy[d, first + k, js].astype(F32), 2 * k + 2, 1)
            last = moved if k == 0 else jnp.where(r3 // 2 == k, moved, last)
        dst[rows, pl.ds(512 * d + 384, 128)] = last.reshape(GR, T).astype(BF)

    def rows_of(d):
        return pl.multiple_of(lax.rem(y + NY - d, NY) * 512, 512)

    def expert_in(g, d):
        slices(g, d)
        assemble(g, d, 0, xm)
        assemble(g, d, 3, cm)
        off = rows_of(d)
        rows = pl.ds(GR * g, GR)
        a = dot(xm[rows, pl.ds(512 * d, 512)], gu[pl.ds(off, 512), :])
        b = dot(cm[rows, pl.ds(512 * d, 512)], dw[:, pl.ds(off, 512)], 1, 1)
        if d == 0:
            acc_gu[rows, :] = a
            acc_h[rows, :] = b
        else:
            acc_gu[rows, :] += a
            acc_h[rows, :] += b

    def activations(g):
        def middle(m, _):
            rows = pl.ds(pl.multiple_of(GR * g + m * 64, 64), 64)
            keep = lax.rem(iota((64, 256), 0), 8) < CAP
            gt = acc_gu[rows, pl.ds(0, 256)]
            u = acc_gu[rows, pl.ds(256, 256)]
            hg = acc_h[rows, :]
            s = jax.nn.sigmoid(gt)
            act = gt * s
            slope = s * (1.0 + gt * (1.0 - s))
            hid[rows, :] = jnp.where(keep, act * u, 0.0).astype(BF)
            gud[rows, pl.ds(0, 256)] = jnp.where(keep, hg * u * slope, 0.0).astype(BF)
            gud[rows, pl.ds(256, 256)] = jnp.where(keep, hg * act, 0.0).astype(BF)
            return 0

        lax.fori_loop(0, GR // 64, middle, 0)

    def packed(g, d, put):
        off = rows_of(d)

        def step(m, _):
            rows = pl.ds(pl.multiple_of(GR * g + m * 128, 128), 128)
            a = dot(gud[rows, :], gu[pl.ds(off, 512), :], 1, 1)
            tail = a[:, 384:512].reshape(16, 8, T)
            rr3 = iota((16, 8, T), 1)
            for k in range(3):
                main = a[:, 128 * k : 128 * k + 128].reshape(16, 8, T)
                put(k, rows, jnp.where(rr3 < CAP, main, pltpu.roll(tail, 6 - 2 * k, 1)))
            return 0

        lax.fori_loop(0, GR // 128, step, 0)

    def put_send(d):
        def put(k, rows, v):
            ps.at[d - 1, k].reshape(512, T)[rows, :] = v.reshape(128, T).astype(BF)

        return put

    def put_own(k, rows, v):
        own[k, rows, :] = v.reshape(128, T)

    HJ = GJ // 2

    def lo(g):
        return pl.ds(GJ * g, HJ)

    def hi(g):
        return pl.ds(GJ * g + HJ, HJ)

    def group(g):
        return pl.ds(GJ * g, GJ)

    def far_partials(g):
        packed(g, 2, put_send(2))
        remote(ps.at[1, :, lo(g)], hl.at[g], rs_send, rs_recv.at[3 * g], right)
        remote(ps.at[1, :, hi(g)], hr.at[g], rs_send, rs_recv.at[3 * g + 1], left)

    def right_partials(g):
        packed(g, 3, put_send(3))
        remote(ps.at[2, :, hi(g)], nl.at[:, hi(g)], rs_send, rs_recv.at[3 * g + 2], right)

    def left_partials(g):
        packed(g, 1, put_send(1))
        remote(ps.at[0, :, lo(g)], nr.at[:, lo(g)], rs_send, rs_recv.at[3 * g + 2], left)

    def merge(g):
        wait(hl.at[g], rs_recv.at[3 * g])
        for k in range(3):
            mrg[0, g, k] = (ps[2, k, lo(g)].astype(F32) + hl[g, k].astype(F32)).astype(BF)
        remote(mrg.at[0, g], nl.at[:, lo(g)], rs_send, rs_recv.at[3 * g + 2], right)
        wait(hr.at[g], rs_recv.at[3 * g + 1])
        for k in range(3):
            mrg[1, g, k] = (ps[0, k, hi(g)].astype(F32) + hr[g, k].astype(F32)).astype(BF)
        remote(mrg.at[1, g], nr.at[:, hi(g)], rs_send, rs_recv.at[3 * g + 2], left)

    def send_back(n, dz, p):
        j = n * PLANE + p
        remote(ret.at[:, j], rr.at[:, j], ret_send, ret_recv.at[n // GC], behind(dz, p) + (y,))

    def give_back(g):
        wait(ps.at[pl.ds(0, 2), :, group(g)], rs_recv.at[3 * g + 2])
        js = pl.ds(GJ * g, GJ)
        for k in range(3):
            total = (
                own[k, pl.ds(GR * g, GR)].reshape(GJ, 8, T)
                + nl[k, js].astype(F32)
                + nr[k, js].astype(F32)
            )
            ret[k, js] = total.astype(BF)
        if g == 0:
            rr[:, 0] = ret[:, 0]
        to_all(send_back, GC * g, GC * g + GC)

    def partials(g):
        activations(g)
        far_partials(g)
        right_partials(g)
        left_partials(g)

    def own_partials(g):
        packed(g, 0, put_own)

    def weight_grad(n):
        cols = pl.ds(256 * n, 256)
        src = pl.multiple_of(lax.rem(y + NY - n // 2, NY) * 512 + (n % 2) * 256, 256)
        both = dot(xm[:, cols], gud[...], 0, 0).astype(BF)
        gg_o[0, pl.ds(src, 256), :] = both[:, :256]
        ug_o[0, pl.ds(src, 256), :] = both[:, 256:]
        dg_o[0, :, pl.ds(src, 256)] = dot(hid[...], cm[:, cols], 0, 0).astype(BF)

    arrived(0)
    arrived(1)
    forward(0)
    arrived(2)
    forward(1)
    loaded(7)
    loaded(8)
    loaded(9)
    expert_in(0, 0)
    expert_in(0, 1)
    expert_in(0, 3)
    arrived(3)
    forward(2)
    expert_in(0, 2)
    partials(0)
    arrived(4)
    forward(3)
    expert_in(1, 0)
    expert_in(1, 1)
    expert_in(1, 3)
    arrived(5)
    forward(4)
    merge(0)
    expert_in(1, 2)
    partials(1)
    own_partials(0)
    arrived(6)
    forward(5)
    arrived(7)
    frecv[0] = fsend[plane]
    to_all(send_fade)
    send_plane(sstw, 0)
    for p in range(1, PLANE):
        remote(ga.at[0], ga.at[p], ga_send, ga_recv, ahead(0, p) + (y,))
    forward(6)
    expert_in(2, 0)
    expert_in(2, 1)
    expert_in(2, 3)
    forward(7)
    merge(1)
    expert_in(2, 2)
    partials(2)
    own_partials(1)
    fades_here()
    plane_totals(0, 0)
    plane_totals(0, 1)
    expert_in(3, 0)
    expert_in(3, 1)
    expert_in(3, 3)
    give_back(0)
    expert_in(3, 2)
    partials(3)
    own_partials(2)
    merge(2)
    own_partials(3)
    give_back(1)
    weight_grad(0)
    weight_grad(1)
    merge(3)
    weight_grad(2)
    give_back(2)
    weight_grad(3)
    give_back(3)
    spread(0, 0, wsw)
    spread(0, 1, wsw)

    for n in range(4, 6):
        weight_grad(n)
    common_t = dot(sw[...], sr[...], 1, 1)
    for h in range(HEADS):
        lst[h] = (lker[h] * common_t).astype(BF)

    moe = None
    for g in range(GROUPS):
        if g == 0:
            wait(rr.at[:, pl.ds(1, GJ - 1)], ret_recv.at[0])
        else:
            wait(rr.at[:, pl.ds(GJ * g, GJ)], ret_recv.at[g])
        cs = slice(GR * g, GR * g + GR)
        parts = []
        tail = None
        for k in range(3):
            both = jnp.concatenate([comb[0, :, cs], comb[1 + k, :, cs]], axis=0)
            v = dot(both, rr.at[k].reshape(512, T)[pl.ds(GR * g, GR), :])
            parts.append(v[:T])
            tail = v[T:] if k == 0 else tail + v[T:]
        parts.append(tail)
        moe = parts if g == 0 else [m + q for m, q in zip(moe, parts)]
    for k in range(4):
        lg[0, :, 128 * k : 128 * k + 128] = (
            cot[:, 128 * k : 128 * k + 128].astype(F32) + moe[k]
        ).astype(BF)
    first = pl.ds(0, 64)
    second = pl.ds(64, 64)
    remote(lg.at[0, first], lg.at[1, first], lg_send, lg_recv.at[0], right)
    remote(lg.at[0, second], lg.at[3, second], lg_send, lg_recv.at[1], left)
    remote(lg.at[0, second], lg.at[1, second], lg_send, lg_recv.at[2], right)
    remote(lg.at[0, first], lg.at[3, first], lg_send, lg_recv.at[3], left)
    loaded(10)

    def out_part(d):
        v = dot(lg[d], pw[pl.ds(rows_of(d), 512), :])
        if d == 0:
            od[...] = v
        else:
            od[...] += v

    def transposed(d):
        yy = lax.rem(y + NY - d, NY)
        for q in range(4):
            blkt = lg[d, :, 128 * q : 128 * q + 128].astype(F32).T.astype(BF)
            lt[yy * 2 + q // 2, pl.ds(4 * (q % 2), 4)] = blkt.reshape(4, 32, T)
        pair = pl.ds(yy * 2, 2)
        for p in range(1, PLANE):
            zz, xx, cc = ahead(0, p)
            remote(
                lt.at[pair, xx * NC + cc], rtm.at[pair, :, pl.ds(T * p, T)], rt_send, rt_recv.at[d],
                (zz, xx, cc, y),
            )
        rtm[pair, :, 0:T] = lt[pair, plane]

    def projection(d):
        yy = lax.rem(y + NY - d, NY)
        pair = pl.ds(yy * 2, 2)
        wait(rtm.at[pair, :, pl.ds(T, T * (PLANE - 1))], rt_recv.at[d])
        pg = dot(rtm[pair].reshape(64, 1024), ga[...].reshape(1024, W)).reshape(2, 32, W)
        pgown[pair] = pg
        pgs[pair] = pg.astype(BF)
        for k in range(2):
            zz = yy * 2 + k

            @pl.when(zz != z)
            def _():
                remote(
                    pgs.at[zz], zr.at[lax.rem(zz + NZ - z, NZ)], z_send, z_recv, (zz, x, c, y)
                )

    out_part(0)
    weight_grad(6)
    weight_grad(7)
    wait(lg.at[1, first], lg_recv.at[0])
    remote(lg.at[1, first], lg.at[2, first], lg_send, lg_recv.at[4], right)
    wait(lg.at[3, second], lg_recv.at[1])
    remote(lg.at[3, second], lg.at[2, second], lg_send, lg_recv.at[5], left)
    transposed(0)
    wait(lg.at[1, second], lg_recv.at[2])
    wait(lg.at[3, first], lg_recv.at[3])
    out_part(1)
    out_part(3)
    transposed(1)
    transposed(3)
    wait(lg.at[2, first], lg_recv.at[4])
    wait(lg.at[2, second], lg_recv.at[5])
    out_part(2)
    odf = od[...].astype(BF).astype(F32)
    ogf = og[...].astype(F32)
    sig = jax.nn.sigmoid(ogf)
    delta = odf * (ogf * sig)
    od[...] = delta
    dl[...] = delta.astype(BF)

    sides(lambda k: od[:, 128 * k : 128 * k + 128], dfs, dfi)
    srt = sr[...].astype(F32).T.astype(BF)
    states(srt, dfs, sstr)
    send_plane(sstr, 1)
    transposed(2)
    og_o[...] = (odf * ms[...].astype(F32) * (sig * (1.0 + ogf * (1.0 - sig)))).astype(BF)

    wsum = None
    for h in range(HEADS):
        cols = slice(128 * (h // 2), 128 * (h // 2) + 128)
        mine = half if h % 2 == 0 else ~half
        dm = jnp.where(mine, od[:, cols], 0.0).astype(BF)
        part = lker[h] * dot(dm, hv[:, cols], 1, 1)
        wsum = part if h == 0 else wsum + part
    rgrad = dot(wsum.astype(BF), sw[...])
    wgrad = dot(wsum.T.astype(BF), sr[...])
    for k in range(HEADS // 2):
        cols = slice(128 * k, 128 * k + 128)
        a = dot(lst[2 * k], dl[:, cols])
        b = dot(lst[2 * k + 1], dl[:, cols])
        vint[:, cols] = jnp.where(half, a, b)
    wait(ga.at[pl.ds(1, PLANE - 1)], ga_recv)
    projection(0)
    plane_totals(1, 0)
    plane_totals(1, 1)
    got_states(wsw, 0)
    for h in range(HEADS):
        rgrad = rgrad + dot(dfi[h], wsw[h], 1, 1)
    rg_o[...] = rgrad.astype(BF)

    projection(1)
    projection(3)
    projection(2)
    spread(1, 0, wsr)
    spread(1, 1, wsr)
    got_states(wsr, 1)
    for k in range(HEADS // 2):
        cols = slice(128 * k, 128 * k + 128)
        u = []
        for h in (2 * k, 2 * k + 1):
            state = wsr[h]
            p = dot(sw[...], state) * fts[h]
            u.append(p + pltpu.roll(p, 64, 1))
            wgrad = wgrad + dot(vfi[h], state, 1, 1)
        vg_o[:, cols] = (vint[:, cols] + jnp.where(half, u[0], u[1])).astype(BF)
    wg_o[...] = wgrad.astype(BF)

    wait(zr.at[pl.ds(1, NZ - 1)], z_recv)
    total = pgown[z]
    for dz in range(1, NZ):
        total = total + zr[dz].astype(F32)
    pg_o[...] = total

    wait(sx.at[:, pl.ds(1, NSP - 1)], d_send)
    wait(gy.at[pl.ds(1, 3)], y_send)
    wait(ps, rs_send)
    wait(ret.at[:, pl.ds(1, NSP - 1)], ret_send)
    wait(lg.at[pl.ds(0, 3)], lg_send)
    wait(inb.at[:, :, pl.ds(1, PLANE - 1)], st_send.at[0])
    wait(zb.at[:, :, pl.ds(1, NZ - 1)], st_send.at[1])
    wait(outb.at[:, :, pl.ds(1, PLANE - 1)], st_send.at[2])
    wait(frecv.at[pl.ds(1, NSP - 1)], fade_send)
    wait(ga.at[pl.ds(1, PLANE - 1)], ga_send)
    wait(rtm.at[:, :, pl.ds(T, T * (PLANE - 1))], rt_send)
    wait(zr.at[pl.ds(1, NZ - 1)], z_send)


def bf(*shape):
    return pltpu.VMEM(shape, BF)


def fl(*shape):
    return pltpu.VMEM(shape, F32)


def sem(n):
    return pltpu.SemaphoreType.DMA((n,))


SCRATCH = (
    pltpu.VMEM((2, T), jnp.int32),
    fl(2, T),
    fl(8, T),
    bf(T, W),
    bf(T, W),
    bf(2048, 512),
    bf(256, 2048),
    bf(T, W),
    bf(T, W),
    bf(T, W),
    bf(2048, 512),
    bf(T, T),
    bf(T, T),
    bf(6, 64, 8, T),
    bf(4, 6, 64, 8, T),
    bf(512, 2048),
    bf(512, 2048),
    fl(512, 512),
    fl(512, 256),
    bf(512, 512),
    bf(512, 256),
    bf(3, 3, 64, 8, T),
    fl(3, 512, T),
    bf(GROUPS, 3, GJ // 2, 8, T),
    bf(GROUPS, 3, GJ // 2, 8, T),
    bf(2, GROUPS, 3, GJ // 2, 8, T),
    bf(3, 64, 8, T),
    bf(3, 64, 8, T),
    bf(3, 64, 8, T),
    bf(3, 64, 8, T),
    bf(4, T, 512),
    bf(4, T, W),
    fl(T, W),
    bf(T, W),
    bf(8, T, T),
    bf(8, T, T),
    fl(8, 64, T),
    bf(2, 2, 8, 64, T),
    bf(2, 2, 2, 32, T),
    bf(2, 2, 8, 32, T),
    bf(2, 2, 8, 64, T),
    fl(8, 1, T),
    pltpu.SemaphoreType.DMA,
    pltpu.SemaphoreType.DMA,
    bf(8, T, T),
    bf(8, T, T),
    fl(8, 1, T),
    fl(64, 1, T),
    bf(8, T, T),
    bf(8, T, T),
    bf(8, T, T),
    bf(8, T, T),
    fl(8, T, T),
    bf(8, T, T),
    fl(8, T, T),
    fl(T, W),
    bf(8, 8, 32, T),
    bf(8, 32, 1024),
    bf(8, T, W),
    bf(8, 32, W),
    bf(8, 32, W),
    fl(8, 32, W),
    sem(14),
    pltpu.SemaphoreType.DMA,
    sem(8),
    pltpu.SemaphoreType.DMA,
    sem(8),
    sem(8),
    sem(GROUPS),
    pltpu.SemaphoreType.DMA,
    sem(3 * GROUPS),
    pltpu.SemaphoreType.DMA,
    sem(GROUPS),
    pltpu.SemaphoreType.DMA,
    sem(6),
    sem(3),
    sem(12),
    pltpu.SemaphoreType.DMA,
    pltpu.SemaphoreType.DMA,
    pltpu.SemaphoreType.DMA,
    sem(4),
    pltpu.SemaphoreType.DMA,
    pltpu.SemaphoreType.DMA,
)


def on_device(
    layer_input, cotangent, routes, route_weight, gate_weight, up_weight, down_weight, heads_value,
    output_gate, mixer_saved, proj_weight, state_write, state_read, decay_rate,
):
    hbm = pl.BlockSpec(memory_space=pl.ANY)
    vmem = pl.BlockSpec(memory_space=pltpu.VMEM)
    shapes = (
        ((1, 2048, 256), BF), ((1, 2048, 256), BF), ((1, 256, 2048), BF), ((32, W), F32),
        ((T, W), BF), ((T, T), BF), ((T, T), BF), ((T, W), BF),
    )
    results = pl.pallas_call(
        body,
        name="layer_backward",
        out_shape=tuple(pltpu.VMEM(s, t) for s, t in shapes),
        in_specs=[hbm] * 14,
        out_specs=tuple([vmem] * 8),
        scratch_shapes=SCRATCH,
        compiler_params=pltpu.CompilerParams(
            collective_id=0, has_side_effects=True, vmem_limit_bytes=52 * 1024 * 1024
        ),
    )(
        layer_input, cotangent, routes.T, route_weight.T, gate_weight, up_weight, down_weight,
        heads_value, output_gate, mixer_saved, proj_weight, state_write, state_read, decay_rate.T,
    )

    def store(*refs):
        sems = refs[-1]
        copies = [
            pltpu.make_async_copy(refs[n], refs[8 + n], sems.at[n]) for n in range(8)
        ]
        for copy in copies:
            copy.start()
        for copy in copies:
            copy.wait()

    return pl.pallas_call(
        store,
        name="store",
        out_shape=tuple(jax.ShapeDtypeStruct(s, t) for s, t in shapes),
        in_specs=[vmem] * 8,
        out_specs=tuple([hbm] * 8),
        scratch_shapes=[sem(8)],
        compiler_params=pltpu.CompilerParams(vmem_limit_bytes=8 * 1024 * 1024),
    )(*results)


def solution(mesh):
    split = Mesh(mesh.devices.reshape(NZ, NX, NC, mesh.shape["tp"]), SP + ("tp",))
    rows, cut = P(SP, None), P(SP, "tp")
    return jax.shard_map(
        on_device,
        mesh=split,
        in_specs=(
            cut, cut, rows, rows, P(SP, None, "tp"), P(SP, None, "tp"), P(SP, "tp", None), cut, cut,
            cut, P(None, "tp"), cut, cut, cut,
        ),
        out_specs=(
            P(SP, None, "tp"), P(SP, None, "tp"), P(SP, "tp", None), cut, cut, cut, cut, cut,
        ),
        check_vma=False,
    )
```

```python
import jax
import jax.numpy as jnp
from jax import lax
from jax.experimental import pallas as pl
from jax.experimental.pallas import tpu as pltpu
from jax.sharding import Mesh
from jax.sharding import PartitionSpec as P

SP = ("sp_0", "sp_1", "sp_2")
NZ, NX, NC, NY = 8, 4, 2, 4
NSP = NZ * NX * NC
PLANE = NX * NC
T = 128
W = 512
HEADS = 8
CAP = 6
BF = jnp.bfloat16
F32 = jnp.float32
ORDER = (0, 1, 6, 3, 5, 4, 2, 7)
PACKED = sum(d << (3 * n) for n, d in enumerate(ORDER))
PLACES = sum(n << (3 * d) for n, d in enumerate(ORDER))
GROUPS = 4
GC = NZ // GROUPS
GJ = GC * PLANE
GR = GJ * 8
MESH_ID = pl.DeviceIdType.MESH
HIGH = lax.Precision.HIGHEST


def dot(a, b, ca=1, cb=0, precision=None):
    return lax.dot_general(
        a, b, (((ca,), (cb,)), ((), ())), preferred_element_type=F32, precision=precision
    )


def iota(shape, dim):
    return lax.broadcasted_iota(jnp.int32, shape, dim)


def body(
    li_h, cot_h, rt_h, rw_h, gw_h, uw_h, dw_h, hv_h, og_h, ms_h, pw_h, sw_h, sr_h, dr_h,
    gg_o, ug_o, dg_o, pg_o, vg_o, wg_o, rg_o, og_o,
    *scratch,
):
    (
        rt_v, rw_v, dr_v, li, cot, gu, dw, hv, og, ms, pw, sw, sr, sx, gy, xm, cm, acc_gu, acc_h, gud, hid, ps,
        own, hl, hr, mrg, nl, nr, ret, rr, comb, lg, od, dl, sstw, sstr, low, inb, zs, zb, outb, fplane, fade_send, fade_recv,
        wsw, wsr, fsend, frecv, vfs, vfi, dfs, dfi, fts, lst, lker, vint, lt, rtm,
        ga, pgs, zr, pgown, ld_sem,
        d_send, d_recv, y_send, yl_recv, yr_recv, yo_recv, rs_send, rs_recv, ret_send, ret_recv,
        lg_send, lg_recv, st_send, st_recv, ga_send, ga_recv, rt_send, rt_recv, z_send, z_recv,
    ) = scratch
    z = lax.axis_index("sp_0")
    x = lax.axis_index("sp_1")
    c = lax.axis_index("sp_2")
    y = lax.axis_index("tp")
    plane = x * NC + c
    me = z * PLANE + plane

    def ahead(dz, p):
        return (
            lax.rem(z + dz, NZ),
            lax.rem(x + p // NC, NX),
            lax.rem(c + p % NC, NC),
        )

    def behind(dz, p):
        return (
            lax.rem(z + NZ - dz, NZ),
            lax.rem(x + NX - p // NC, NX),
            lax.rem(c + p % NC, NC),
        )

    right = (z, x, c, lax.rem(y + 1, NY))
    left = (z, x, c, lax.rem(y + NY - 1, NY))

    def remote(src, dst, ss, rs, dev):
        pltpu.make_async_remote_copy(
            src_ref=src, dst_ref=dst, send_sem=ss, recv_sem=rs, device_id=dev,
            device_id_type=MESH_ID,
        ).start()

    def local(src, dst, sem):
        pltpu.make_async_copy(src, dst, sem).start()

    def wait(ref, sem):
        pltpu.make_async_copy(ref, ref, sem).wait()

    def dz_of(n):
        return lax.shift_right_logical(jnp.int32(PACKED), 3 * n) & 7

    def n_of(dz):
        return lax.shift_right_logical(jnp.int32(PLACES), 3 * dz) & 7

    def dz_vec(n):
        out = jnp.zeros_like(n)
        for k, d in enumerate(ORDER):
            out = jnp.where(n == k, d, out)
        return out

    def to_all(send, first=0, last=NZ):
        if first == 0:
            for p in range(1, PLANE):
                send(0, 0, p)

        def step(n, _):
            dz = dz_of(n)
            for p in range(PLANE):
                send(n, dz, p)
            return 0

        lax.fori_loop(max(first, 1), last, step, 0)

    loads = (
        (li_h, li), (cot_h, cot), (hv_h, hv), (sw_h, sw), (sr_h, sr), (og_h, og), (ms_h, ms),
        (gw_h.at[0], gu.at[:, pl.ds(0, 256)]), (uw_h.at[0], gu.at[:, pl.ds(256, 256)]),
        (dw_h.at[0], dw), (pw_h, pw), (rt_h, rt_v), (rw_h, rw_v), (dr_h, dr_v),
    )
    for n in (11, 12, 13, 0, 1, 2, 3, 4, 5, 6, 7, 8, 9, 10):
        local(*loads[n], ld_sem.at[n])

    def loaded(n):
        wait(loads[n][1], ld_sem.at[n])

    bar = pltpu.get_barrier_semaphore()

    def greet(dev):
        pl.semaphore_signal(bar, inc=1, device_id=dev, device_id_type=MESH_ID)

    to_all(lambda n, dz, p: greet(ahead(dz, p) + (y,)))
    greet(right)
    greet(left)

    for e in range(2):
        for u in range(2):
            zb[e, u, 0] = jnp.zeros((32, T), BF)
    loaded(11)
    loaded(12)
    loaded(13)
    ci = iota((512, T), 0)
    r8 = lax.rem(ci, 8)
    blk = ci // 8
    e = (
        lax.rem(z + dz_vec(blk // PLANE), NZ) * PLANE
        + lax.rem(x + lax.rem(blk // NC, NX), NX) * NC
        + lax.rem(c + lax.rem(blk, NC), NC)
    )
    r0 = jnp.broadcast_to(rt_v[0:1, :], (512, T))
    r1 = jnp.broadcast_to(rt_v[1:2, :], (512, T))
    hit = (r0 == e) | (r1 == e)
    upper = (iota((T, T), 0) < iota((T, T), 1)).astype(F32).astype(BF)
    hitf = jnp.where(hit, 1.0, 0.0)
    rank = dot(hitf.astype(BF), upper).astype(jnp.int32)
    wsel = jnp.where(
        r0 == e, jnp.broadcast_to(rw_v[0:1, :], (512, T)), jnp.broadcast_to(rw_v[1:2, :], (512, T))
    )
    base = hit & (rank == r8) & (r8 < CAP)
    basef = jnp.where(base, 1.0, 0.0)
    extra = [
        jnp.where(hit & (rank == 2 * k + r8 - CAP) & (r8 >= CAP), 1.0, 0.0) for k in range(3)
    ]
    loaded(0)
    loaded(1)
    for k in range(3):
        pick = jnp.concatenate([basef.astype(BF), extra[k].astype(BF)], axis=1)
        rows = jnp.concatenate(
            [
                jnp.concatenate([li[:, 128 * k : 128 * k + 128], cot[:, 128 * k : 128 * k + 128]], axis=1),
                jnp.concatenate([li[:, 384:512], cot[:, 384:512]], axis=1),
            ],
            axis=0,
        )
        got = dot(pick, rows)
        weight = jnp.sum((basef + extra[k]) * wsel, axis=1, keepdims=True)
        sx.at[k].reshape(512, T)[...] = got[:, :128].astype(BF)
        sx.at[3 + k].reshape(512, T)[...] = (got[:, 128:] * weight).astype(BF)

    comb[0] = basef.T.astype(BF)
    for k in range(3):
        comb[1 + k] = extra[k].T.astype(BF)

    loaded(2)
    loaded(3)
    loaded(4)
    upto = (iota((T, T), 0) <= iota((T, T), 1)).astype(F32)
    cum = dot(dr_v[...], upto, precision=HIGH)
    tot = cum[:, 127:128]
    te = jnp.exp(cum - tot)
    ts = jnp.exp(-cum)
    stacked = jnp.concatenate([te, ts, cum, jnp.zeros((T - 24, T), F32)], axis=0)
    tr = stacked.T
    half = iota((T, T), 1) < 64
    for h in range(HEADS):
        fsend[h] = jnp.broadcast_to(jnp.exp(-tot[h : h + 1, :]), (1, T))
        te_c = jnp.broadcast_to(tr[:, h : h + 1], (T, T))
        ts_c = jnp.broadcast_to(tr[:, 8 + h : 9 + h], (T, T))
        fts[h] = jnp.where(half, ts_c, te_c)
        cc = jnp.broadcast_to(tr[:, 16 + h : 17 + h], (T, T))
        cr = jnp.broadcast_to(cum[h : h + 1, :], (T, T))
        lker[h] = jnp.exp(-jnp.abs(cc - cr))

    def doubled(v, h):
        other = pltpu.roll(v, 64, 1)
        return jnp.where(half, v, other) if h % 2 == 0 else jnp.where(half, other, v)

    def sides(chunk_of, first, second):
        for h in range(HEADS):
            v = doubled(chunk_of(h // 2), h)
            f = fts[h]
            second[h] = (v * f).astype(BF)
            first[h] = (v * pltpu.roll(f, 64, 1)).astype(BF)

    sides(lambda k: hv[:, 128 * k : 128 * k + 128].astype(F32), vfs, vfi)

    def states(vectors_t, first, dst):
        for h in range(0, HEADS, 2):
            s = dot(vectors_t, jnp.concatenate([first[h], first[h + 1]], axis=1))
            dst[h] = s[:, :T].astype(BF)
            dst[h + 1] = s[:, T:].astype(BF)

    swt = sw[...].astype(F32).T.astype(BF)
    states(swt, vfs, sstw)

    def place(i):
        return lax.rem(x + NX - i // NC, NX) * NC + lax.rem(c + i % NC, NC)

    def rowhalf(u):
        return pl.ds(64 * u, 64)

    quarter = iota((32, T), 1) < 64

    def packed_half(v, at_left):
        other = pltpu.roll(v[:32] if not at_left else v[32:], 64, 1)
        return jnp.where(quarter, v[:32] if at_left else other, other if at_left else v[32:])

    def send_plane(src, e):
        for u in range(2):
            k = 6 * e + 3 * u
            for p in range(1, PLANE):
                zz, xx, cc = ahead(0, p)
                remote(
                    src.at[xx * NC + cc, rowhalf(u)], inb.at[e, u, p], st_send.at[0], st_recv.at[k],
                    (zz, xx, cc, y),
                )
            inb[e, u, 0] = src[plane, rowhalf(u)]

    def plane_totals(e, u):
        k = 6 * e + 3 * u
        wait(inb.at[e, u, pl.ds(1, PLANE - 1)], st_recv.at[k])
        up = None
        down = None
        for i in range(PLANE):
            p = place(i)
            q = place(PLANE - 1 - i)
            v = inb[e, u, p].astype(F32)
            w = inb[e, u, q].astype(F32)
            up = v if i == 0 else up * frecv[p] + v
            down = w if i == 0 else down * frecv[q] + w
        zs[e, u, 0] = packed_half(up, True).astype(BF)
        zs[e, u, 1] = packed_half(down, False).astype(BF)
        for dz in (4, 5, 3, 6, 2, 1, 7):
            zz = lax.rem(z + dz, NZ)
            remote(
                zs.at[e, u, (z + dz) // NZ], zb.at[e, u, dz], st_send.at[1], st_recv.at[k + 1],
                (zz, x, c, y),
            )

    def spread(e, u, dst):
        k = 6 * e + 3 * u
        wait(zb.at[e, u, pl.ds(1, NZ - 1)], st_recv.at[k + 1])
        up = jnp.zeros((32, T), F32)
        down = jnp.zeros((32, T), F32)
        for i in range(NZ):
            dz = lax.rem(z + NZ - i, NZ)
            f = fplane[n_of(dz)]
            v = zb[e, u, dz].astype(F32)
            up = jnp.where((z - i + NZ - 1) // NZ == 1, up * f + v, up)
            r = NZ - 1 - i
            dz = lax.rem(z + NZ - r, NZ)
            f = fplane[n_of(dz)]
            v = zb[e, u, dz].astype(F32)
            down = jnp.where((r - z + NZ - 1) // NZ == 1, down * f + v, down)
        start = jnp.concatenate(
            [
                jnp.where(quarter, up, pltpu.roll(down, 64, 1)),
                jnp.where(quarter, pltpu.roll(up, 64, 1), down),
            ],
            axis=0,
        )
        cur = start
        for i in range(PLANE):
            p = place(i)
            low[p] = cur
            if i < PLANE - 1:
                cur = cur * frecv[p] + inb[e, u, p].astype(F32)
        cur = start
        for i in reversed(range(PLANE)):
            p = place(i)
            outb[e, u, p] = jnp.where(half[:64], low[p], cur).astype(BF)
            if i > 0:
                cur = cur * frecv[p] + inb[e, u, p].astype(F32)
        for p in range(1, PLANE):
            zz, xx, cc = behind(0, p)
            remote(
                outb.at[e, u, p], dst.at[plane, rowhalf(u)], st_send.at[2], st_recv.at[k + 2],
                (zz, xx, cc, y),
            )
        dst[plane, rowhalf(u)] = outb[e, u, 0]

    def got_states(ref, e):
        for u in range(2):
            wait(inb.at[e, u, pl.ds(1, PLANE - 1)], st_recv.at[6 * e + 3 * u + 2])

    def fades_here():
        wait(frecv.at[pl.ds(1, NSP - 1)], fade_recv)
        for n in range(NZ):
            f = frecv[PLANE * n]
            for p in range(1, PLANE):
                f = f * frecv[PLANE * n + p]
            fplane[n] = f

    def send_fade(n, dz, p):
        zz, xx, cc = ahead(dz, p)
        j = n * PLANE + p
        remote(fsend.at[xx * NC + cc], frecv.at[j], fade_send, fade_recv, (zz, xx, cc, y))

    loaded(5)
    loaded(6)
    ogf = og[...].astype(F32)
    sig = jax.nn.sigmoid(ogf)
    ga[0] = (ms[...].astype(F32) * (ogf * sig)).astype(BF)
    pl.semaphore_wait(bar, NSP - 1 + 2)

    def send_x(n, dz, p):
        j = n * PLANE + p
        remote(sx.at[:, j], gy.at[0, :, j], d_send, d_recv.at[n], ahead(dz, p) + (y,))

    gy[0, :, 0] = sx[:, 0]
    to_all(send_x)

    def chunk(d, n):
        return gy.at[d, :, pl.ds(PLANE * n, PLANE)]

    def forward(n):
        if n % 2 == 0:
            wait(chunk(1, n), yl_recv.at[n])
            remote(chunk(1, n), chunk(2, n), y_send, yo_recv.at[n // GC], right)
        else:
            wait(chunk(3, n), yr_recv.at[n])
            remote(chunk(3, n), chunk(2, n), y_send, yo_recv.at[n // GC], left)

    def arrived(n):
        if n == 0:
            wait(gy.at[0, :, pl.ds(1, PLANE - 1)], d_recv.at[0])
        else:
            wait(chunk(0, n), d_recv.at[n])
        remote(chunk(0, n), chunk(1, n), y_send, yl_recv.at[n], right)
        remote(chunk(0, n), chunk(3, n), y_send, yr_recv.at[n], left)

    def slices(g, d):
        for n in range(GC * g, GC * g + GC):
            if d == 1 and n % 2 == 1:
                wait(chunk(1, n), yl_recv.at[n])
            if d == 3 and n % 2 == 0:
                wait(chunk(3, n), yr_recv.at[n])
        if d == 2:
            wait(gy.at[2, :, pl.ds(GJ * g, GJ)], yo_recv.at[g])

    r3 = iota((GJ, 8, T), 1)

    def assemble(g, d, first, dst):
        last = None
        rows = pl.ds(GR * g, GR)
        js = pl.ds(GJ * g, GJ)
        for k in range(3):
            dst[rows, pl.ds(512 * d + 128 * k, 128)] = gy.at[d, first + k].reshape(512, T)[rows, :]
            moved = pltpu.roll(gy[d, first + k, js].astype(F32), 2 * k + 2, 1)
            last = moved if k == 0 else jnp.where(r3 // 2 == k, moved, last)
        dst[rows, pl.ds(512 * d + 384, 128)] = last.reshape(GR, T).astype(BF)

    def rows_of(d):
        return pl.multiple_of(lax.rem(y + NY - d, NY) * 512, 512)

    def expert_in(g, d):
        slices(g, d)
        assemble(g, d, 0, xm)
        assemble(g, d, 3, cm)
        off = rows_of(d)
        rows = pl.ds(GR * g, GR)
        a = dot(xm[rows, pl.ds(512 * d, 512)], gu[pl.ds(off, 512), :])
        b = dot(cm[rows, pl.ds(512 * d, 512)], dw[:, pl.ds(off, 512)], 1, 1)
        if d == 0:
            acc_gu[rows, :] = a
            acc_h[rows, :] = b
        else:
            acc_gu[rows, :] += a
            acc_h[rows, :] += b

    def activations(g):
        def middle(m, _):
            rows = pl.ds(pl.multiple_of(GR * g + m * 64, 64), 64)
            keep = lax.rem(iota((64, 256), 0), 8) < CAP
            gt = acc_gu[rows, pl.ds(0, 256)]
            u = acc_gu[rows, pl.ds(256, 256)]
            hg = acc_h[rows, :]
            s = jax.nn.sigmoid(gt)
            act = gt * s
            slope = s * (1.0 + gt * (1.0 - s))
            hid[rows, :] = jnp.where(keep, act * u, 0.0).astype(BF)
            gud[rows, pl.ds(0, 256)] = jnp.where(keep, hg * u * slope, 0.0).astype(BF)
            gud[rows, pl.ds(256, 256)] = jnp.where(keep, hg * act, 0.0).astype(BF)
            return 0

        lax.fori_loop(0, GR // 64, middle, 0)

    def packed(g, d, put):
        off = rows_of(d)

        def step(m, _):
            rows = pl.ds(pl.multiple_of(GR * g + m * 128, 128), 128)
            a = dot(gud[rows, :], gu[pl.ds(off, 512), :], 1, 1)
            tail = a[:, 384:512].reshape(16, 8, T)
            rr3 = iota((16, 8, T), 1)
            for k in range(3):
                main = a[:, 128 * k : 128 * k + 128].reshape(16, 8, T)
                put(k, rows, jnp.where(rr3 < CAP, main, pltpu.roll(tail, 6 - 2 * k, 1)))
            return 0

        lax.fori_loop(0, GR // 128, step, 0)

    def put_send(d):
        def put(k, rows, v):
            ps.at[d - 1, k].reshape(512, T)[rows, :] = v.reshape(128, T).astype(BF)

        return put

    def put_own(k, rows, v):
        own[k, rows, :] = v.reshape(128, T)

    HJ = GJ // 2

    def lo(g):
        return pl.ds(GJ * g, HJ)

    def hi(g):
        return pl.ds(GJ * g + HJ, HJ)

    def group(g):
        return pl.ds(GJ * g, GJ)

    def far_partials(g):
        packed(g, 2, put_send(2))
        remote(ps.at[1, :, lo(g)], hl.at[g], rs_send, rs_recv.at[3 * g], right)
        remote(ps.at[1, :, hi(g)], hr.at[g], rs_send, rs_recv.at[3 * g + 1], left)

    def right_partials(g):
        packed(g, 3, put_send(3))
        remote(ps.at[2, :, hi(g)], nl.at[:, hi(g)], rs_send, rs_recv.at[3 * g + 2], right)

    def left_partials(g):
        packed(g, 1, put_send(1))
        remote(ps.at[0, :, lo(g)], nr.at[:, lo(g)], rs_send, rs_recv.at[3 * g + 2], left)

    def merge(g):
        wait(hl.at[g], rs_recv.at[3 * g])
        for k in range(3):
            mrg[0, g, k] = (ps[2, k, lo(g)].astype(F32) + hl[g, k].astype(F32)).astype(BF)
        remote(mrg.at[0, g], nl.at[:, lo(g)], rs_send, rs_recv.at[3 * g + 2], right)
        wait(hr.at[g], rs_recv.at[3 * g + 1])
        for k in range(3):
            mrg[1, g, k] = (ps[0, k, hi(g)].astype(F32) + hr[g, k].astype(F32)).astype(BF)
        remote(mrg.at[1, g], nr.at[:, hi(g)], rs_send, rs_recv.at[3 * g + 2], left)

    def send_back(n, dz, p):
        j = n * PLANE + p
        remote(ret.at[:, j], rr.at[:, j], ret_send, ret_recv.at[n // GC], behind(dz, p) + (y,))

    def give_back(g):
        wait(ps.at[pl.ds(0, 2), :, group(g)], rs_recv.at[3 * g + 2])
        js = pl.ds(GJ * g, GJ)
        for k in range(3):
            total = (
                own[k, pl.ds(GR * g, GR)].reshape(GJ, 8, T)
                + nl[k, js].astype(F32)
                + nr[k, js].astype(F32)
            )
            ret[k, js] = total.astype(BF)
        if g == 0:
            rr[:, 0] = ret[:, 0]
        to_all(send_back, GC * g, GC * g + GC)

    def partials(g):
        activations(g)
        far_partials(g)
        right_partials(g)
        left_partials(g)

    def own_partials(g):
        packed(g, 0, put_own)

    def weight_grad(n):
        cols = pl.ds(256 * n, 256)
        src = pl.multiple_of(lax.rem(y + NY - n // 2, NY) * 512 + (n % 2) * 256, 256)
        both = dot(xm[:, cols], gud[...], 0, 0).astype(BF)
        gg_o[0, pl.ds(src, 256), :] = both[:, :256]
        ug_o[0, pl.ds(src, 256), :] = both[:, 256:]
        dg_o[0, :, pl.ds(src, 256)] = dot(hid[...], cm[:, cols], 0, 0).astype(BF)

    arrived(0)
    arrived(1)
    forward(0)
    arrived(2)
    forward(1)
    loaded(7)
    loaded(8)
    loaded(9)
    expert_in(0, 0)
    expert_in(0, 1)
    expert_in(0, 3)
    arrived(3)
    forward(2)
    expert_in(0, 2)
    partials(0)
    arrived(4)
    forward(3)
    expert_in(1, 0)
    expert_in(1, 1)
    expert_in(1, 3)
    arrived(5)
    forward(4)
    merge(0)
    expert_in(1, 2)
    partials(1)
    own_partials(0)
    arrived(6)
    forward(5)
    arrived(7)
    frecv[0] = fsend[plane]
    to_all(send_fade)
    send_plane(sstw, 0)
    for p in range(1, PLANE):
        remote(ga.at[0], ga.at[p], ga_send, ga_recv, ahead(0, p) + (y,))
    forward(6)
    expert_in(2, 0)
    expert_in(2, 1)
    expert_in(2, 3)
    forward(7)
    merge(1)
    expert_in(2, 2)
    partials(2)
    own_partials(1)
    fades_here()
    plane_totals(0, 0)
    plane_totals(0, 1)
    expert_in(3, 0)
    expert_in(3, 1)
    expert_in(3, 3)
    give_back(0)
    expert_in(3, 2)
    partials(3)
    own_partials(2)
    merge(2)
    own_partials(3)
    give_back(1)
    weight_grad(0)
    weight_grad(1)
    merge(3)
    weight_grad(2)
    give_back(2)
    weight_grad(3)
    give_back(3)

    for n in range(4, 6):
        weight_grad(n)
    common_t = dot(sw[...], sr[...], 1, 1)
    for h in range(HEADS):
        lst[h] = (lker[h] * common_t).astype(BF)

    moe = None
    for g in range(GROUPS):
        if g == 0:
            wait(rr.at[:, pl.ds(1, GJ - 1)], ret_recv.at[0])
        else:
            wait(rr.at[:, pl.ds(GJ * g, GJ)], ret_recv.at[g])
        cs = slice(GR * g, GR * g + GR)
        parts = []
        tail = None
        for k in range(3):
            both = jnp.concatenate([comb[0, :, cs], comb[1 + k, :, cs]], axis=0)
            v = dot(both, rr.at[k].reshape(512, T)[pl.ds(GR * g, GR), :])
            parts.append(v[:T])
            tail = v[T:] if k == 0 else tail + v[T:]
        parts.append(tail)
        moe = parts if g == 0 else [m + q for m, q in zip(moe, parts)]
    for k in range(4):
        lg[0, :, 128 * k : 128 * k + 128] = (
            cot[:, 128 * k : 128 * k + 128].astype(F32) + moe[k]
        ).astype(BF)
    first = pl.ds(0, 64)
    second = pl.ds(64, 64)
    remote(lg.at[0, first], lg.at[1, first], lg_send, lg_recv.at[0], right)
    remote(lg.at[0, second], lg.at[3, second], lg_send, lg_recv.at[1], left)
    remote(lg.at[0, second], lg.at[1, second], lg_send, lg_recv.at[2], right)
    remote(lg.at[0, first], lg.at[3, first], lg_send, lg_recv.at[3], left)
    loaded(10)

    def out_part(d):
        v = dot(lg[d], pw[pl.ds(rows_of(d), 512), :])
        if d == 0:
            od[...] = v
        else:
            od[...] += v

    def transposed(d):
        yy = lax.rem(y + NY - d, NY)
        for q in range(4):
            blkt = lg[d, :, 128 * q : 128 * q + 128].astype(F32).T.astype(BF)
            lt[yy * 2 + q // 2, pl.ds(4 * (q % 2), 4)] = blkt.reshape(4, 32, T)
        pair = pl.ds(yy * 2, 2)
        for p in range(1, PLANE):
            zz, xx, cc = ahead(0, p)
            remote(
                lt.at[pair, xx * NC + cc], rtm.at[pair, :, pl.ds(T * p, T)], rt_send, rt_recv.at[d],
                (zz, xx, cc, y),
            )
        rtm[pair, :, 0:T] = lt[pair, plane]

    def projection(d):
        yy = lax.rem(y + NY - d, NY)
        pair = pl.ds(yy * 2, 2)
        wait(rtm.at[pair, :, pl.ds(T, T * (PLANE - 1))], rt_recv.at[d])
        pg = dot(rtm[pair].reshape(64, 1024), ga[...].reshape(1024, W)).reshape(2, 32, W)
        pgown[pair] = pg
        pgs[pair] = pg.astype(BF)
        for k in range(2):
            zz = yy * 2 + k

            @pl.when(zz != z)
            def _():
                remote(
                    pgs.at[zz], zr.at[lax.rem(zz + NZ - z, NZ)], z_send, z_recv, (zz, x, c, y)
                )

    out_part(0)
    spread(0, 0, wsw)
    spread(0, 1, wsw)
    weight_grad(6)
    weight_grad(7)
    wait(lg.at[1, first], lg_recv.at[0])
    remote(lg.at[1, first], lg.at[2, first], lg_send, lg_recv.at[4], right)
    wait(lg.at[3, second], lg_recv.at[1])
    remote(lg.at[3, second], lg.at[2, second], lg_send, lg_recv.at[5], left)
    transposed(0)
    wait(lg.at[1, second], lg_recv.at[2])
    wait(lg.at[3, first], lg_recv.at[3])
    out_part(1)
    out_part(3)
    transposed(1)
    transposed(3)
    wait(lg.at[2, first], lg_recv.at[4])
    wait(lg.at[2, second], lg_recv.at[5])
    out_part(2)
    odf = od[...].astype(BF).astype(F32)
    ogf = og[...].astype(F32)
    sig = jax.nn.sigmoid(ogf)
    delta = odf * (ogf * sig)
    od[...] = delta
    dl[...] = delta.astype(BF)

    for h in range(HEADS):
        v = doubled(od[:, 128 * (h // 2) : 128 * (h // 2) + 128], h)
        dfs[h] = (v * pltpu.roll(fts[h], 64, 1)).astype(BF)
    srt = sr[...].astype(F32).T.astype(BF)
    states(srt, dfs, sstr)
    send_plane(sstr, 1)
    transposed(2)
    for h in range(HEADS):
        v = doubled(od[:, 128 * (h // 2) : 128 * (h // 2) + 128], h)
        dfi[h] = (v * fts[h]).astype(BF)
    og_o[...] = (odf * ms[...].astype(F32) * (sig * (1.0 + ogf * (1.0 - sig)))).astype(BF)

    wsum = None
    for h in range(HEADS):
        cols = slice(128 * (h // 2), 128 * (h // 2) + 128)
        mine = half if h % 2 == 0 else ~half
        dm = jnp.where(mine, od[:, cols], 0.0).astype(BF)
        part = lker[h] * dot(dm, hv[:, cols], 1, 1)
        wsum = part if h == 0 else wsum + part
    rgrad = dot(wsum.astype(BF), sw[...])
    wgrad = dot(wsum.T.astype(BF), sr[...])
    for k in range(HEADS // 2):
        cols = slice(128 * k, 128 * k + 128)
        a = dot(lst[2 * k], dl[:, cols])
        b = dot(lst[2 * k + 1], dl[:, cols])
        vint[:, cols] = jnp.where(half, a, b)
    wait(ga.at[pl.ds(1, PLANE - 1)], ga_recv)
    projection(0)
    plane_totals(1, 0)
    plane_totals(1, 1)
    got_states(wsw, 0)
    for h in range(HEADS):
        rgrad = rgrad + dot(dfi[h], wsw[h], 1, 1)
    rg_o[...] = rgrad.astype(BF)

    projection(1)
    projection(3)
    projection(2)
    spread(1, 0, wsr)
    spread(1, 1, wsr)
    got_states(wsr, 1)
    for k in range(HEADS // 2):
        cols = slice(128 * k, 128 * k + 128)
        u = []
        for h in (2 * k, 2 * k + 1):
            state = wsr[h]
            p = dot(sw[...], state) * fts[h]
            u.append(p + pltpu.roll(p, 64, 1))
            wgrad = wgrad + dot(vfi[h], state, 1, 1)
        vg_o[:, cols] = (vint[:, cols] + jnp.where(half, u[0], u[1])).astype(BF)
    wg_o[...] = wgrad.astype(BF)

    wait(zr.at[pl.ds(1, NZ - 1)], z_recv)
    total = pgown[z]
    for dz in range(1, NZ):
        total = total + zr[dz].astype(F32)
    pg_o[...] = total

    wait(sx.at[:, pl.ds(1, NSP - 1)], d_send)
    wait(gy.at[pl.ds(1, 3)], y_send)
    wait(ps, rs_send)
    wait(ret.at[:, pl.ds(1, NSP - 1)], ret_send)
    wait(lg.at[pl.ds(0, 3)], lg_send)
    wait(inb.at[:, :, pl.ds(1, PLANE - 1)], st_send.at[0])
    wait(zb.at[:, :, pl.ds(1, NZ - 1)], st_send.at[1])
    wait(outb.at[:, :, pl.ds(1, PLANE - 1)], st_send.at[2])
    wait(frecv.at[pl.ds(1, NSP - 1)], fade_send)
    wait(ga.at[pl.ds(1, PLANE - 1)], ga_send)
    wait(rtm.at[:, :, pl.ds(T, T * (PLANE - 1))], rt_send)
    wait(zr.at[pl.ds(1, NZ - 1)], z_send)


def bf(*shape):
    return pltpu.VMEM(shape, BF)


def fl(*shape):
    return pltpu.VMEM(shape, F32)


def sem(n):
    return pltpu.SemaphoreType.DMA((n,))


SCRATCH = (
    pltpu.VMEM((2, T), jnp.int32),
    fl(2, T),
    fl(8, T),
    bf(T, W),
    bf(T, W),
    bf(2048, 512),
    bf(256, 2048),
    bf(T, W),
    bf(T, W),
    bf(T, W),
    bf(2048, 512),
    bf(T, T),
    bf(T, T),
    bf(6, 64, 8, T),
    bf(4, 6, 64, 8, T),
    bf(512, 2048),
    bf(512, 2048),
    fl(512, 512),
    fl(512, 256),
    bf(512, 512),
    bf(512, 256),
    bf(3, 3, 64, 8, T),
    fl(3, 512, T),
    bf(GROUPS, 3, GJ // 2, 8, T),
    bf(GROUPS, 3, GJ // 2, 8, T),
    bf(2, GROUPS, 3, GJ // 2, 8, T),
    bf(3, 64, 8, T),
    bf(3, 64, 8, T),
    bf(3, 64, 8, T),
    bf(3, 64, 8, T),
    bf(4, T, 512),
    bf(4, T, W),
    fl(T, W),
    bf(T, W),
    bf(8, T, T),
    bf(8, T, T),
    fl(8, 64, T),
    bf(2, 2, 8, 64, T),
    bf(2, 2, 2, 32, T),
    bf(2, 2, 8, 32, T),
    bf(2, 2, 8, 64, T),
    fl(8, 1, T),
    pltpu.SemaphoreType.DMA,
    pltpu.SemaphoreType.DMA,
    bf(8, T, T),
    bf(8, T, T),
    fl(8, 1, T),
    fl(64, 1, T),
    bf(8, T, T),
    bf(8, T, T),
    bf(8, T, T),
    bf(8, T, T),
    fl(8, T, T),
    bf(8, T, T),
    fl(8, T, T),
    fl(T, W),
    bf(8, 8, 32, T),
    bf(8, 32, 1024),
    bf(8, T, W),
    bf(8, 32, W),
    bf(8, 32, W),
    fl(8, 32, W),
    sem(14),
    pltpu.SemaphoreType.DMA,
    sem(8),
    pltpu.SemaphoreType.DMA,
    sem(8),
    sem(8),
    sem(GROUPS),
    pltpu.SemaphoreType.DMA,
    sem(3 * GROUPS),
    pltpu.SemaphoreType.DMA,
    sem(GROUPS),
    pltpu.SemaphoreType.DMA,
    sem(6),
    sem(3),
    sem(12),
    pltpu.SemaphoreType.DMA,
    pltpu.SemaphoreType.DMA,
    pltpu.SemaphoreType.DMA,
    sem(4),
    pltpu.SemaphoreType.DMA,
    pltpu.SemaphoreType.DMA,
)


def on_device(
    layer_input, cotangent, routes, route_weight, gate_weight, up_weight, down_weight, heads_value,
    output_gate, mixer_saved, proj_weight, state_write, state_read, decay_rate,
):
    hbm = pl.BlockSpec(memory_space=pl.ANY)
    vmem = pl.BlockSpec(memory_space=pltpu.VMEM)
    shapes = (
        ((1, 2048, 256), BF), ((1, 2048, 256), BF), ((1, 256, 2048), BF), ((32, W), F32),
        ((T, W), BF), ((T, T), BF), ((T, T), BF), ((T, W), BF),
    )
    results = pl.pallas_call(
        body,
        name="layer_backward",
        out_shape=tuple(pltpu.VMEM(s, t) for s, t in shapes),
        in_specs=[hbm] * 14,
        out_specs=tuple([vmem] * 8),
        scratch_shapes=SCRATCH,
        compiler_params=pltpu.CompilerParams(
            collective_id=0, has_side_effects=True, vmem_limit_bytes=52 * 1024 * 1024
        ),
    )(
        layer_input, cotangent, routes.T, route_weight.T, gate_weight, up_weight, down_weight,
        heads_value, output_gate, mixer_saved, proj_weight, state_write, state_read, decay_rate.T,
    )

    def store(*refs):
        sems = refs[-1]
        copies = [
            pltpu.make_async_copy(refs[n], refs[8 + n], sems.at[n]) for n in range(8)
        ]
        for copy in copies:
            copy.start()
        for copy in copies:
            copy.wait()

    return pl.pallas_call(
        store,
        name="store",
        out_shape=tuple(jax.ShapeDtypeStruct(s, t) for s, t in shapes),
        in_specs=[vmem] * 8,
        out_specs=tuple([hbm] * 8),
        scratch_shapes=[sem(8)],
        compiler_params=pltpu.CompilerParams(vmem_limit_bytes=8 * 1024 * 1024),
    )(*results)


def solution(mesh):
    split = Mesh(mesh.devices.reshape(NZ, NX, NC, mesh.shape["tp"]), SP + ("tp",))
    rows, cut = P(SP, None), P(SP, "tp")
    return jax.shard_map(
        on_device,
        mesh=split,
        in_specs=(
            cut, cut, rows, rows, P(SP, None, "tp"), P(SP, None, "tp"), P(SP, "tp", None), cut, cut,
            cut, P(None, "tp"), cut, cut, cut,
        ),
        out_specs=(
            P(SP, None, "tp"), P(SP, None, "tp"), P(SP, "tp", None), cut, cut, cut, cut, cut,
        ),
        check_vma=False,
    )
```
